128 devices in a mesh: fs: 16 (over z, x), tp: 8 (over y, core).
Axes of the slice: x: 4, y: 4, z: 4, core: 2. Of those that a mesh axis runs over, the one named last changes fastest.
Arguments:
- resid: bfloat16 [16384, 2048], P(('fs', 'tp')), may hold values from -6 to 6
- mix_gain: float32 [2048], replicated, may hold values from 0.1 to 1.9
- in_weight: bfloat16 [2048, 2048], P('fs', 'tp'), may hold values from -0.125 to 0.125
- conv_taps: float32 [4, 2048], P(None, 'tp'), may hold values from -3 to 3
- recur_gate_w: bfloat16 [32, 64, 64], P('tp'), may hold values from -0.75 to 0.75
- input_gate_w: bfloat16 [32, 64, 64], P('tp'), may hold values from -0.75 to 0.75
- decay_rate: float32 [2048], P('tp'), may hold values from 0.0004 to 0.03
- out_weight: bfloat16 [2048, 2048], P('tp', 'fs'), may hold values from -0.25 to 0.25
- mlp_gain: float32 [2048], replicated, may hold values from 0.1 to 1.9
- up_gate_w: bfloat16 [2048, 5632], P('fs', 'tp'), may hold values from -0.125 to 0.125
- up_val_w: bfloat16 [2048, 5632], P('fs', 'tp'), may hold values from -0.125 to 0.125
- ffn_taps: float32 [3, 5632], P(None, 'tp'), may hold values from -3 to 3
- down_weight: bfloat16 [5632, 2048], P('tp', 'fs'), may hold values from -0.15625 to 0.15625
Outputs:
- result: bfloat16 [16384, 2048], P(('fs', 'tp'))
The draws below stay inside these ranges and needn't reach their ends.
All inputs are finite; a program needn't handle non-finite values.
Results may differ from the reference program's by a relative error of at most 0.028.
Values may be sent and summed in bfloat16 or wider, within the bound.
A program may use at most 64 MiB of HBM per device.

```python
import math
import jax
import jax.numpy as jnp
from jax import lax

D = 2048
RECUR = 2048
HIDDEN_SIZE = 5632
GATE_BLOCK = 64
SEQ_LEN = 128
NBLOCKS = 32
TOKENS = 16384
N_TP = 8


def block_levels(stream_key, dims, pieces, low, high):
    gain = 1.0
    for position, parts in pieces:
        heights = jax.random.uniform(jax.random.fold_in(jax.random.fold_in(stream_key, 6), position), (parts,), jnp.float32, low / len(pieces), high / len(pieces))
        gain = gain * jnp.repeat(jnp.exp(heights), dims[position] // parts).reshape((-1,) + (1,) * (len(dims) - 1 - position))
    return gain


def noise(rng, dims, spread, reach, shards=(), kind=jnp.bfloat16):
    level = block_levels(rng, dims, shards, -0.22, 0.18) if shards else 1.0
    drawn = jax.random.normal(rng, dims, jnp.float32) * spread * level
    return jnp.minimum(jnp.maximum(drawn, -reach), reach).astype(kind)


def setup_inputs(seed: int = 0) -> dict:
    splits = jax.random.split(jax.random.key(seed), 14)
    return {
        "resid": noise(splits[0], (TOKENS, D), 1.0, 6.0, ((0, 128),)),
        "mix_gain": jnp.clip(1.0 + 0.18 * jax.random.normal(splits[1], (D,), jnp.float32), 0.1, 1.9),
        "in_weight": noise(splits[2], (D, RECUR), D ** -0.5, 0.125, ((0, 16), (1, 8))),
        "conv_taps": noise(splits[3], (4, RECUR), 0.5, 3.0, ((1, 8),), jnp.float32),
        "recur_gate_w": noise(splits[4], (NBLOCKS, GATE_BLOCK, GATE_BLOCK), GATE_BLOCK ** -0.5, 0.75, ((0, 8),)),
        "input_gate_w": noise(splits[5], (NBLOCKS, GATE_BLOCK, GATE_BLOCK), GATE_BLOCK ** -0.5, 0.75, ((0, 8),)),
        "decay_rate": jnp.clip(jnp.exp(math.log(0.03) - 4.317488 * jax.random.uniform(splits[6], (RECUR,), jnp.float32) ** block_levels(splits[6], (RECUR,), ((0, 8),), -0.2, 0.2)), 0.0004, 0.03),
        "out_weight": noise(splits[7], (RECUR, D), (RECUR // 4) ** -0.5, 0.25, ((0, 8), (1, 16))),
        "mlp_gain": jnp.clip(1.0 + 0.18 * jax.random.normal(splits[8], (D,), jnp.float32), 0.1, 1.9),
        "up_gate_w": noise(splits[9], (D, HIDDEN_SIZE), D ** -0.5, 0.125, ((0, 16), (1, 8))),
        "up_val_w": noise(splits[10], (D, HIDDEN_SIZE), D ** -0.5, 0.125, ((0, 16), (1, 8))),
        "ffn_taps": noise(splits[11], (3, HIDDEN_SIZE), 0.6, 3.0, ((1, 8),), jnp.float32),
        "down_weight": noise(splits[12], (HIDDEN_SIZE, D), (HIDDEN_SIZE // 4) ** -0.5, 0.15625, ((0, 8), (1, 16))),
    }


def rms_scale(rows_in, gain_vec):
    wide = rows_in.astype(jnp.float32)
    return wide * lax.rsqrt(lax.optimization_barrier(jnp.mean(wide * wide, axis=-1, keepdims=True)) + 1e-06) * gain_vec

def causal_taps(values, tap_weights):
    width = tap_weights.shape[0]
    length = values.shape[1]
    padded = jnp.pad(values, ((0, 0), (width - 1, 0), (0, 0)))
    summed = jnp.zeros_like(values)
    for tap_index in range(width):
        summed = summed + padded[:, tap_index:tap_index + length] * tap_weights[tap_index]
    return summed

def combine(earlier, later):
    return (earlier[0] * later[0], later[0] * earlier[1] + later[1])

def group_sum(left, right, groups):
    step_size = left.shape[1] // groups
    summed = jnp.zeros((left.shape[0], right.shape[1]), jnp.float32)
    for group in range(groups):
        term = jnp.dot(left[:, group * step_size:(group + 1) * step_size], right[group * step_size:(group + 1) * step_size], preferred_element_type=jnp.float32)
        term = lax.optimization_barrier(term.astype(jnp.bfloat16))
        summed = summed + term.astype(jnp.float32)
    return summed

def reference(resid, mix_gain, in_weight, conv_taps, recur_gate_w, input_gate_w, decay_rate, out_weight, mlp_gain, up_gate_w, up_val_w, ffn_taps, down_weight):
    seqs = TOKENS // SEQ_LEN
    normed = rms_scale(resid, mix_gain).astype(jnp.bfloat16)
    projected = jnp.dot(normed, in_weight, preferred_element_type=jnp.float32).astype(jnp.bfloat16)
    conv = causal_taps(projected.astype(jnp.float32).reshape(seqs, SEQ_LEN, RECUR), conv_taps)
    blocks = conv.astype(jnp.bfloat16).astype(jnp.float32).reshape(seqs, SEQ_LEN, NBLOCKS, GATE_BLOCK)
    rgate = jax.nn.sigmoid(jnp.einsum('slnd,nde->slne', blocks, recur_gate_w.astype(jnp.float32)).reshape(seqs, SEQ_LEN, RECUR))
    igate = jax.nn.sigmoid(jnp.einsum('slnd,nde->slne', blocks, input_gate_w.astype(jnp.float32)).reshape(seqs, SEQ_LEN, RECUR))
    logdecay = -8.0 * rgate * decay_rate
    decay = jnp.exp(logdecay)
    drive = jnp.sqrt(-jnp.expm1(2.0 * logdecay)) * (igate * conv)
    state = lax.associative_scan(combine, (decay, drive), axis=1)[1]
    recurred = state.astype(jnp.bfloat16).reshape(TOKENS, RECUR)
    mixed_sum = group_sum(recurred, out_weight, N_TP)
    middle = (resid.astype(jnp.float32) + mixed_sum).astype(jnp.bfloat16)
    normed_two = rms_scale(middle, mlp_gain).astype(jnp.bfloat16)
    gate_pre = jnp.dot(normed_two, up_gate_w, preferred_element_type=jnp.float32).astype(jnp.bfloat16)
    value_pre = jnp.dot(normed_two, up_val_w, preferred_element_type=jnp.float32).astype(jnp.bfloat16)
    gate_conv = causal_taps(gate_pre.astype(jnp.float32).reshape(seqs, SEQ_LEN, HIDDEN_SIZE), ffn_taps).reshape(TOKENS, HIDDEN_SIZE)
    hidden = (jax.nn.silu(gate_conv) * value_pre.astype(jnp.float32)).astype(jnp.bfloat16)
    ffn_sum = group_sum(hidden, down_weight, N_TP)
    return (middle.astype(jnp.float32) + ffn_sum).astype(jnp.bfloat16)
```

```python
import jax
import jax.numpy as jnp
from jax import lax
from jax.experimental import pallas as pl
from jax.experimental.pallas import tpu as pltpu
from jax.sharding import Mesh
from jax.sharding import PartitionSpec as P

GATE_BLOCK = 64
SEQ = 128
HALF = 64
RING = 4
MESH = pl.DeviceIdType.MESH
BF16 = jnp.bfloat16
F32 = jnp.float32

OWN, RIGHT, LEFT, FAR, IN_RIGHT, IN_LEFT, IN_FAR = 0, 2, 4, 6, 8, 10, 12


def remote(src, dst, send_sem, recv_sem, **device):
    return pltpu.make_async_remote_copy(
        src_ref=src,
        dst_ref=dst,
        send_sem=send_sem,
        recv_sem=recv_sem,
        device_id=device,
        device_id_type=MESH,
    )


def far_order(k):
    return lax.rem(k * (k + 1) // 2, RING)


def rms_rows(wide, gain):
    scale = lax.rsqrt(jnp.mean(wide * wide, axis=-1, keepdims=True) + 1e-06)
    return (wide * scale * gain).astype(BF16)


def shifted(values, rows, by, fill):
    return jnp.where(rows >= by, pltpu.roll(values, by, axis=0), fill)


def kernel(
    resid,
    mix_gain,
    in_w,
    conv_taps,
    recur_w,
    input_w,
    decay_rate,
    out_w,
    mlp_gain,
    up_w,
    ffn_taps,
    down_w,
    result,
    in_g,
    out_g,
    up_g,
    down_g,
    rows_g,
    gate_w,
    proj,
    gates,
    recurred,
    pre,
    hidden,
    partial,
    from_core,
    to_ring,
    far_in,
    near_in,
    middle,
    w_send,
    w_recv,
    w_local,
    g_send,
    g_recv,
    c_send,
    c_recv,
    r_send,
    r_recv,
):
    z, x, y, c = (lax.axis_index(a) for a in ("z", "x", "y", "c"))
    at = {"z": z, "x": x, "y": y}

    def nxt(axis, by):
        return lax.rem(at[axis] + (by + RING), RING)

    other = 1 - c
    y_right, y_left, y_far = nxt("y", 1), nxt("y", -1), nxt("y", 2)

    barrier = pltpu.get_barrier_semaphore()
    for axis in ("z", "x", "y"):
        for by in (1, -1):
            pl.semaphore_signal(
                barrier, inc=1, device_id={axis: nxt(axis, by)}, device_id_type=MESH
            )
    pl.semaphore_signal(barrier, inc=1, device_id={"c": other}, device_id_type=MESH)
    pl.semaphore_wait(barrier, 7)

    weights = ((in_w, in_g), (out_w, out_g), (up_w, up_g), (down_w, down_g))

    def piece(i, p):
        rows = weights[i][1].shape[2] // 4
        return pl.ds(p * rows, rows)

    def axes_of(p):
        return ("x", "z") if p < 2 else ("z", "x")

    def slot(i, p, axis, by):
        g = weights[i][1]
        if axis == "x":
            return g.at[z, nxt("x", by), piece(i, p)]
        return g.at[nxt("z", by), x, piece(i, p)]

    def line(i, p, axis, by):
        g = weights[i][1]
        if axis == "z":
            return g.at[nxt("z", by), :, piece(i, p)]
        return g.at[:, nxt("x", by), piece(i, p)]

    def w_copy(i, p, src, dst, k, axis, by):
        return remote(src, dst, w_send.at[i, p, k], w_recv.at[i, p, k], **{axis: nxt(axis, by)})

    def own_copy(i):
        src, g = weights[i]
        return pltpu.make_async_copy(src, g.at[z, x], w_local.at[i])

    def first_send(i):
        src = weights[i][0]
        for p in range(4):
            axis = axes_of(p)[0]
            for k, by in ((0, 1), (1, -1)):
                w_copy(i, p, src.at[piece(i, p)], slot(i, p, axis, 0), k, axis, by).start()

    def first_wait(i, p, k):
        axis = axes_of(p)[0]
        by = (-1, 1, 2)[k]
        there = slot(i, p, axis, by)
        w_copy(i, p, there, there, k, axis, 1).wait_recv()

    def first_forward(i):
        for p in range(4):
            axis = axes_of(p)[0]
            k = p % 2
            first_wait(i, p, k)
            by = 1 if k == 0 else -1
            there = slot(i, p, axis, -by)
            w_copy(i, p, there, there, 2, axis, by).start()

    def second_send(i):
        own_copy(i).wait()
        for p in range(4):
            axis = axes_of(p)[1]
            first_wait(i, p, 1 - p % 2)
            first_wait(i, p, 2)
            here = line(i, p, axis, 0)
            for k, by in ((3, 1), (4, -1)):
                w_copy(i, p, here, here, k, axis, by).start()

    def second_wait(i, p, k):
        axis = axes_of(p)[1]
        by = (-1, 1, 2)[k - 3]
        there = line(i, p, axis, by)
        w_copy(i, p, there, there, k, axis, 1).wait_recv()

    def second_forward(i):
        for p in range(4):
            axis = axes_of(p)[1]
            k = 3 + p % 2
            second_wait(i, p, k)
            by = 1 if k == 3 else -1
            there = line(i, p, axis, -by)
            w_copy(i, p, there, there, 5, axis, by).start()

    def weights_done(i):
        for p in range(4):
            second_wait(i, p, 4 - p % 2)
            second_wait(i, p, 5)

    def weights_sent(i):
        for p in range(4):
            first, second = axes_of(p)
            one, four = slot(i, p, first, 0), line(i, p, second, 0)
            for k in range(6):
                ref = one if k < 3 else four
                w_copy(i, p, ref, ref, k, first, 1).wait_send()

    def g_copy(n, yq, cq, h, s, r, **device):
        ref = rows_g.at[n, yq, cq, h]
        return remote(ref, ref, g_send.at[n, s], g_recv.at[n, r], **device)

    def rows_wait(n, yq, cq, h, r):
        g_copy(n, yq, cq, h, 0, r, c=other).wait_recv()

    def rows_send(n):
        for h in (0, 1):
            g_copy(n, y, c, h, h, IN_LEFT + h, y=y_right).start()
            g_copy(n, y, c, 1 - h, 2 + 1 - h, IN_RIGHT + 1 - h, y=y_left).start()
            g_copy(n, y, c, h, 4 + h, OWN + h, c=other).start()

    def rows_first(n):
        rows_wait(n, y_left, c, 0, IN_LEFT)
        g_copy(n, y_left, c, 0, 6, IN_FAR, y=y_right).start()
        g_copy(n, y_left, c, 0, 8, LEFT, c=other).start()
        rows_wait(n, y_right, c, 1, IN_RIGHT + 1)
        g_copy(n, y_right, c, 1, 7, IN_FAR + 1, y=y_left).start()
        g_copy(n, y_right, c, 1, 11, RIGHT + 1, c=other).start()

    def rows_second(n):
        rows_wait(n, y_left, c, 1, IN_LEFT + 1)
        g_copy(n, y_left, c, 1, 9, LEFT + 1, c=other).start()
        rows_wait(n, y_right, c, 0, IN_RIGHT)
        g_copy(n, y_right, c, 0, 10, RIGHT, c=other).start()

    def rows_third(n):
        for h in (0, 1):
            rows_wait(n, y_far, c, h, IN_FAR + h)
            g_copy(n, y_far, c, h, 12 + h, FAR + h, c=other).start()

    def rows_sent(n):
        for s in range(14):
            g_copy(n, y, c, 0, s, 0, c=other).wait_send()

    def pair_ready(n, k, yq):
        for h in (0, 1):
            rows_wait(n, yq, other, h, 2 * k + h)

    def core_copy(n, yq, k):
        return remote(
            partial.at[yq, other], from_core.at[n, yq], c_send.at[n, k], c_recv.at[n, k], c=other
        )

    def r_copy(n, src, dst, k, **device):
        return remote(src, dst, r_send.at[n, k], r_recv.at[n, k], **device)

    def chip_sum(n, yq, h, at_row, extra=None):
        rows = pl.ds(h * HALF + at_row, 16)
        total = partial[yq, c, rows, :].astype(F32) + from_core[n, yq, rows, :].astype(F32)
        if extra is not None:
            total = total + extra[pl.ds(at_row, 16), :].astype(F32)
        return total

    def fill_ring(n, j, h, yq, extra=None):
        @pl.loop(0, HALF, step=16)
        def _(at_row):
            at_row = pl.multiple_of(at_row, 16)
            to_ring[n, j, h, pl.ds(at_row, 16), :] = chip_sum(n, yq, h, at_row, extra).astype(BF16)

    def sums_far(n):
        core_copy(n, y_far, 0).wait_recv()
        fill_ring(n, 0, 0, y_far)
        r_copy(n, to_ring.at[n, 0, 0], far_in.at[n, 0], 0, y=y_right).start()
        fill_ring(n, 0, 1, y_far)
        r_copy(n, to_ring.at[n, 0, 1], far_in.at[n, 1], 1, y=y_left).start()

    def sums_left(n):
        core_copy(n, y_left, 1).wait_recv()
        fill_ring(n, 1, 0, y_left)
        r_copy(n, to_ring.at[n, 1, 0], near_in.at[n, 1, 0], 2, y=y_left).start()

    def sums_right(n):
        core_copy(n, y_right, 2).wait_recv()
        fill_ring(n, 2, 1, y_right)
        r_copy(n, to_ring.at[n, 2, 1], near_in.at[n, 0, 1], 3, y=y_right).start()

    def sums_near(n):
        r_copy(n, far_in.at[n, 0], far_in.at[n, 0], 0, y=y_right).wait_recv()
        fill_ring(n, 2, 0, y_right, far_in.at[n, 0])
        r_copy(n, to_ring.at[n, 2, 0], near_in.at[n, 0, 0], 4, y=y_right).start()
        r_copy(n, far_in.at[n, 1], far_in.at[n, 1], 1, y=y_right).wait_recv()
        fill_ring(n, 1, 1, y_left, far_in.at[n, 1])
        r_copy(n, to_ring.at[n, 1, 1], near_in.at[n, 1, 1], 5, y=y_left).start()

    def near_wait(n, side, h):
        k = ((4, 3), (2, 5))[side][h]
        ref = near_in.at[n, side, h]
        r_copy(n, ref, ref, k, y=y_right).wait_recv()

    def sums_sent(n):
        for k in range(4):
            core_copy(n, y, k).wait_send()
        for k in range(6):
            r_copy(n, to_ring.at[n, 0, 0], to_ring.at[n, 0, 0], k, y=y_right).wait_send()

    def sums_wait(n):
        core_copy(n, y, 3).wait_recv()
        for side in (0, 1):
            for h in (0, 1):
                near_wait(n, side, h)

    def own_sum(n, h, at_row):
        total = chip_sum(n, y, h, at_row)
        for side in (0, 1):
            total = total + near_in[n, side, h, pl.ds(at_row, 16), :].astype(F32)
        return total

    for i in range(4):
        own_copy(i).start()
    first_send(0)
    first_send(1)

    for h in (0, 1):

        @pl.loop(0, HALF, step=16)
        def _(at_row):
            at_row = pl.multiple_of(at_row, 16)
            wide = resid[pl.ds(h * HALF + at_row, 16), :].astype(F32)
            rows_g[0, y, c, h, pl.ds(at_row, 16), :] = rms_rows(wide, mix_gain[...])

    rows_send(0)

    gate_w[...] = jnp.zeros_like(gate_w)
    for n in range(recur_w.shape[0]):
        block = slice(n * GATE_BLOCK, (n + 1) * GATE_BLOCK)
        gate_w[block, block] = recur_w[n]
        block_two = slice(256 + n * GATE_BLOCK, 256 + (n + 1) * GATE_BLOCK)
        gate_w[block, block_two] = input_w[n]

    first_forward(0)
    first_forward(1)
    second_send(0)
    second_send(1)
    first_send(2)
    first_send(3)
    rows_first(0)
    second_forward(0)
    second_forward(1)
    rows_second(0)
    first_forward(2)
    first_forward(3)
    weights_done(0)

    @pl.loop(0, RING)
    def _(k):
        @pl.when(k == 2)
        def _():
            second_send(2)

        @pl.when(k == 3)
        def _():
            rows_third(0)

        yq = lax.rem(y + far_order(k), RING)
        pair_ready(0, k, yq)
        columns = rows_g[0, yq].reshape(2 * SEQ, -1)
        w = in_g[...].reshape(-1, 256)
        wide = jnp.dot(columns, w, preferred_element_type=F32)
        wide = wide.astype(BF16).astype(F32)
        rows2 = lax.rem(lax.broadcasted_iota(jnp.int32, wide.shape, 0), SEQ)
        taps = conv_taps[...]
        conv = shifted(wide, rows2, 3, 0.0) * taps[0:1]
        conv = conv + shifted(wide, rows2, 2, 0.0) * taps[1:2]
        conv = conv + shifted(wide, rows2, 1, 0.0) * taps[2:3]
        conv = conv + wide * taps[3:4]
        proj[...] = conv
        gates[...] = jnp.dot(conv.astype(BF16), gate_w[...], preferred_element_type=F32)

        for s in range(2):
            for b in range(2):
                rows = slice(s * SEQ, (s + 1) * SEQ)
                lanes = slice(b * 128, (b + 1) * 128)
                lanes2 = slice(256 + b * 128, 256 + (b + 1) * 128)
                rgate = jax.nn.sigmoid(gates[rows, lanes])
                igate = jax.nn.sigmoid(gates[rows, lanes2])
                a = 8.0 * rgate * decay_rate[:, lanes]
                decay = jnp.exp(-a)
                a2 = a * a
                small = 2.0 * decay * (a * (1.0 + a2 * (1.0 / 6) * (1.0 + a2 * (1.0 / 20) * (1.0 + a2 * (1.0 / 42)))))
                left_over = jnp.where(a < 0.3, small, 1.0 - decay * decay)
                state = jnp.sqrt(left_over) * (igate * proj[rows, lanes])
                pos = lax.broadcasted_iota(jnp.int32, state.shape, 0)
                by = 1
                while by < SEQ:
                    state = decay * shifted(state, pos, by, 0.0) + state
                    if 2 * by < SEQ:
                        decay = decay * shifted(decay, pos, by, 1.0)
                    by *= 2
                recurred[yq, rows, lanes] = state.astype(BF16)

    weights_done(1)
    second_send(3)

    def mixed(yq):
        left = recurred[yq]
        for zq in range(RING):
            w = jnp.concatenate([out_g[zq, xq] for xq in range(RING)], axis=1)
            term = jnp.dot(left, w, preferred_element_type=F32).astype(BF16)
            for s in range(2):
                partial[yq, s, :, zq * 512 : (zq + 1) * 512] = term[s * SEQ : (s + 1) * SEQ]

    def lowered(yq):
        left = hidden[yq]
        for zq in range(RING):
            w = jnp.concatenate([down_g[zq, xq] for xq in range(RING)], axis=1)
            term = jnp.dot(left, w, preferred_element_type=F32).astype(BF16)
            for s in range(2):
                partial[yq, s, :, zq * 512 : (zq + 1) * 512] = term[s * SEQ : (s + 1) * SEQ]

    def summed(n, product):
        @pl.loop(0, RING)
        def _(k):
            yq = lax.rem(y + far_order(RING - 1 - k), RING)
            product(yq)
            core_copy(n, yq, k).start()
            for step, part in ((1, sums_far), (2, sums_left), (3, sums_right)):

                @pl.when(k == step)
                def _():
                    part(n)

        sums_near(n)

    summed(0, mixed)
    second_forward(2)
    sums_wait(0)

    for h in (0, 1):

        @pl.loop(0, HALF, step=16)
        def _(at_row):
            at_row = pl.multiple_of(at_row, 16)
            here = pl.ds(h * HALF + at_row, 16)
            mid = (resid[here, :].astype(F32) + own_sum(0, h, at_row)).astype(BF16)
            middle[here, :] = mid
            rows_g[1, y, c, h, pl.ds(at_row, 16), :] = rms_rows(mid.astype(F32), mlp_gain[...])

    rows_send(1)
    sums_sent(0)
    weights_done(2)

    def gated(gate, value, taps, pos):
        conv = shifted(gate, pos, 2, 0.0) * taps[0:1]
        conv = conv + shifted(gate, pos, 1, 0.0) * taps[1:2]
        conv = conv + gate * taps[2:3]
        return (conv / (1.0 + jnp.exp(-conv)) * value).astype(BF16)

    @pl.loop(0, RING)
    def _(k):
        @pl.when(k == 1)
        def _():
            rows_first(1)
            rows_second(1)

        @pl.when(k == 2)
        def _():
            second_forward(3)

        @pl.when(k == 3)
        def _():
            rows_third(1)

        yq = lax.rem(y + far_order(k), RING)
        pair_ready(1, k, yq)
        columns = rows_g[1, yq].reshape(2 * SEQ, -1)
        w = up_g[...].reshape(-1, 1408)
        pre[...] = jnp.dot(columns, w, preferred_element_type=F32)

        for s in range(2):
            rows = slice(s * SEQ, (s + 1) * SEQ)
            for b in range(6):
                lanes = slice(b * 128, (b + 1) * 128)
                if b < 5:
                    gate = pre[rows, lanes].astype(BF16).astype(F32)
                    value = pre[rows, 640 + b * 128 : 640 + (b + 1) * 128].astype(BF16).astype(F32)
                else:
                    gate = pre[rows, 1280:1408].astype(BF16).astype(F32)
                    value = pltpu.roll(gate, 64, axis=1)
                pos = lax.broadcasted_iota(jnp.int32, gate.shape, 0)
                unit = gated(gate, value, ffn_taps[:, lanes], pos)
                if b < 5:
                    hidden[yq, rows, lanes] = unit
                else:
                    hidden[yq, rows, 640:704] = unit[:, :64]

    weights_done(3)
    summed(1, lowered)
    sums_wait(1)

    for h in (0, 1):

        @pl.loop(0, HALF, step=16)
        def _(at_row):
            at_row = pl.multiple_of(at_row, 16)
            here = pl.ds(h * HALF + at_row, 16)
            result[here, :] = (middle[here, :].astype(F32) + own_sum(1, h, at_row)).astype(BF16)

    sums_sent(1)
    for n in range(2):
        rows_sent(n)
    for i in range(4):
        weights_sent(i)


def shards(
    resid,
    mix_gain,
    in_weight,
    conv_taps,
    recur_gate_w,
    input_gate_w,
    decay_rate,
    out_weight,
    mlp_gain,
    up_gate_w,
    up_val_w,
    ffn_taps,
    down_weight,
):
    up = jnp.concatenate(
        [up_gate_w[:, :640], up_val_w[:, :640], up_gate_w[:, 640:], up_val_w[:, 640:]], axis=1
    )
    taps = jnp.pad(ffn_taps, ((0, 0), (0, 64)))
    vmem = pl.BlockSpec(memory_space=pltpu.VMEM)
    hbm = pl.BlockSpec(memory_space=pl.ANY)
    dma = pltpu.SemaphoreType.DMA
    width = resid.shape[1]
    return pl.pallas_call(
        kernel,
        name="layer",
        out_shape=jax.ShapeDtypeStruct(resid.shape, BF16),
        in_specs=[vmem, vmem, hbm, vmem, vmem, vmem, vmem, hbm, vmem, hbm, vmem, hbm],
        out_specs=vmem,
        scratch_shapes=[
            pltpu.VMEM((RING, RING, *in_weight.shape), BF16),
            pltpu.VMEM((RING, RING, *out_weight.shape), BF16),
            pltpu.VMEM((RING, RING, *up.shape), BF16),
            pltpu.VMEM((RING, RING, *down_weight.shape), BF16),
            pltpu.VMEM((2, RING, 2, 2, HALF, width), BF16),
            pltpu.VMEM((256, 512), BF16),
            pltpu.VMEM((2 * SEQ, 256), F32),
            pltpu.VMEM((2 * SEQ, 512), F32),
            pltpu.VMEM((RING, 2 * SEQ, 256), BF16),
            pltpu.VMEM((2 * SEQ, up.shape[1]), F32),
            pltpu.VMEM((RING, 2 * SEQ, 704), BF16),
            pltpu.VMEM((RING, 2, SEQ, width), BF16),
            pltpu.VMEM((2, RING, SEQ, width), BF16),
            pltpu.VMEM((2, 3, 2, HALF, width), BF16),
            pltpu.VMEM((2, 2, HALF, width), BF16),
            pltpu.VMEM((2, 2, 2, HALF, width), BF16),
            pltpu.VMEM((SEQ, width), BF16),
            dma((4, 4, 6)),
            dma((4, 4, 6)),
            dma((4,)),
            dma((2, 14)),
            dma((2, 14)),
            dma((2, 4)),
            dma((2, 4)),
            dma((2, 6)),
            dma((2, 6)),
        ],
        compiler_params=pltpu.CompilerParams(
            collective_id=0, has_side_effects=True, vmem_limit_bytes=60 * 1024 * 1024
        ),
    )(
        resid,
        mix_gain[None],
        in_weight,
        conv_taps,
        recur_gate_w,
        input_gate_w,
        decay_rate[None],
        out_weight,
        mlp_gain[None],
        up,
        taps,
        down_weight,
    )


def solution(mesh):
    split = Mesh(mesh.devices.reshape(RING, RING, RING, 2), ("z", "x", "y", "c"))
    fs, tp = ("z", "x"), ("y", "c")
    rows = ("z", "x", "y", "c")
    return jax.shard_map(
        shards,
        mesh=split,
        in_specs=(
            P(rows, None),
            P(),
            P(fs, tp),
            P(None, tp),
            P(tp, None, None),
            P(tp, None, None),
            P(tp),
            P(tp, fs),
            P(),
            P(fs, tp),
            P(fs, tp),
            P(None, tp),
            P(tp, fs),
        ),
        out_specs=P(rows, None),
        check_vma=False,
    )
```

```python
import jax
import jax.numpy as jnp
from jax import lax
from jax.experimental import pallas as pl
from jax.experimental.pallas import tpu as pltpu
from jax.sharding import Mesh
from jax.sharding import PartitionSpec as P

GATE_BLOCK = 64
SEQ = 128
HALF = 64
QUARTER = 32
RING = 4
MESH = pl.DeviceIdType.MESH
BF16 = jnp.bfloat16
F32 = jnp.float32

OWN, RIGHT, LEFT, FAR, IN_RIGHT, IN_LEFT, IN_FAR = 0, 2, 4, 6, 8, 10, 12


def remote(src, dst, send_sem, recv_sem, **device):
    return pltpu.make_async_remote_copy(
        src_ref=src,
        dst_ref=dst,
        send_sem=send_sem,
        recv_sem=recv_sem,
        device_id=device,
        device_id_type=MESH,
    )


def rms_rows(wide, gain):
    scale = lax.rsqrt(jnp.mean(wide * wide, axis=-1, keepdims=True) + 1e-06)
    return (wide * scale * gain).astype(BF16)


def shifted(values, rows, by, fill):
    return jnp.where(rows >= by, pltpu.roll(values, by, axis=0), fill)


def behind(extended, by):
    return pltpu.roll(extended, by, axis=0)[8:]


def kernel(
    resid_hbm,
    mix_gain,
    in_w,
    conv_taps,
    recur_w,
    input_w,
    decay_rate,
    out_w,
    mlp_gain,
    gate_t,
    value_t,
    ffn_taps,
    down_w,
    result,
    resid,
    gate_in,
    value_in,
    in_g,
    out_g,
    up_g,
    down_g,
    rows_g,
    gate_w,
    proj,
    gates,
    conv_tail,
    carry,
    recurred,
    pre,
    gate_tail,
    hidden,
    partial,
    from_core,
    to_ring,
    far_in,
    near_in,
    middle,
    w_send,
    w_recv,
    l_sem,
    g_send,
    g_recv,
    c_send,
    c_recv,
    r_send,
    r_recv,
):
    z, x, y, c = (lax.axis_index(a) for a in ("z", "x", "y", "c"))
    at = {"z": z, "x": x, "y": y}

    def nxt(axis, by):
        return lax.rem(at[axis] + (by + RING), RING)

    other = 1 - c
    y_right, y_left, y_far = nxt("y", 1), nxt("y", -1), nxt("y", 2)

    weights = ((in_w, in_g), (out_w, out_g), (None, up_g), (down_w, down_g))

    def own_copy(i):
        if i < 4:
            src, g = weights[i]
            return pltpu.make_async_copy(src, g.at[z, x], l_sem.at[i])
        src, dst = ((resid_hbm, resid), (gate_t, gate_in), (value_t, value_in))[i - 4]
        return pltpu.make_async_copy(src, dst, l_sem.at[i])

    for i in (4, 5, 6, 0, 1, 3):
        own_copy(i).start()

    barrier = pltpu.get_barrier_semaphore()
    for axis in ("z", "x", "y"):
        for by in (1, -1):
            pl.semaphore_signal(
                barrier, inc=1, device_id={axis: nxt(axis, by)}, device_id_type=MESH
            )
    pl.semaphore_signal(barrier, inc=1, device_id={"c": other}, device_id_type=MESH)
    pl.semaphore_wait(barrier, 7)

    def piece(i, p):
        rows = weights[i][1].shape[2] // 4
        return pl.ds(p * rows, rows)

    def axes_of(p):
        return ("x", "z") if p < 2 else ("z", "x")

    def slot(i, p, axis, by):
        g = weights[i][1]
        if axis == "x":
            return g.at[z, nxt("x", by), piece(i, p)]
        return g.at[nxt("z", by), x, piece(i, p)]

    def line(i, p, axis, by):
        g = weights[i][1]
        if axis == "z":
            return g.at[nxt("z", by), :, piece(i, p)]
        return g.at[:, nxt("x", by), piece(i, p)]

    def w_copy(i, p, src, dst, k, axis, by):
        return remote(src, dst, w_send.at[i, p, k], w_recv.at[i, p, k], **{axis: nxt(axis, by)})

    def first_send(i):
        src = weights[i][0]
        for p in range(4):
            axis = axes_of(p)[0]
            here = slot(i, p, axis, 0)
            for k, by in ((0, 1), (1, -1)):
                w_copy(i, p, here if src is None else src.at[piece(i, p)], here, k, axis, by).start()

    def first_wait(i, p, k):
        axis = axes_of(p)[0]
        there = slot(i, p, axis, (-1, 1, 2)[k])
        w_copy(i, p, there, there, k, axis, 1).wait_recv()

    def first_forward(i):
        for p in range(4):
            axis = axes_of(p)[0]
            k = p % 2
            first_wait(i, p, k)
            by = 1 if k == 0 else -1
            there = slot(i, p, axis, -by)
            w_copy(i, p, there, there, 2, axis, by).start()

    def second_send(i):
        if weights[i][0] is not None:
            own_copy(i).wait()
        for p in range(4):
            axis = axes_of(p)[1]
            first_wait(i, p, 1 - p % 2)
            first_wait(i, p, 2)
            here = line(i, p, axis, 0)
            for k, by in ((3, 1), (4, -1)):
                w_copy(i, p, here, here, k, axis, by).start()

    def second_wait(i, p, k):
        axis = axes_of(p)[1]
        there = line(i, p, axis, (-1, 1, 2)[k - 3])
        w_copy(i, p, there, there, k, axis, 1).wait_recv()

    def second_forward(i):
        for p in range(4):
            axis = axes_of(p)[1]
            k = 3 + p % 2
            second_wait(i, p, k)
            by = 1 if k == 3 else -1
            there = line(i, p, axis, -by)
            w_copy(i, p, there, there, 5, axis, by).start()

    def weights_done(i):
        for p in range(4):
            second_wait(i, p, 4 - p % 2)
            second_wait(i, p, 5)

    def weights_sent(i):
        for p in range(4):
            first, second = axes_of(p)
            one, four = slot(i, p, first, 0), line(i, p, second, 0)
            for k in range(6):
                ref = one if k < 3 else four
                w_copy(i, p, ref, ref, k, first, 1).wait_send()

    def g_copy(n, yq, cq, q, s, r, **device):
        ref = rows_g.at[n, yq, cq, q]
        return remote(ref, ref, g_send.at[n, s], g_recv.at[n, r], **device)

    def rows_wait(n, yq, cq, q, r):
        g_copy(n, yq, cq, q, 0, r, c=other).wait_recv()

    def rows_send(n):
        for q in (0, 1):
            g_copy(n, y, c, q, q, IN_LEFT + q, y=y_right).start()
            g_copy(n, y, c, 1 - q, 2 + 1 - q, IN_RIGHT + 1 - q, y=y_left).start()
            g_copy(n, y, c, q, 4 + q, OWN + q, c=other).start()

    def rows_first(n):
        rows_wait(n, y_left, c, 0, IN_LEFT)
        g_copy(n, y_left, c, 0, 6, IN_FAR, y=y_right).start()
        g_copy(n, y_left, c, 0, 8, LEFT, c=other).start()
        rows_wait(n, y_right, c, 1, IN_RIGHT + 1)
        g_copy(n, y_right, c, 1, 7, IN_FAR + 1, y=y_left).start()
        g_copy(n, y_right, c, 1, 11, RIGHT + 1, c=other).start()

    def rows_second(n):
        rows_wait(n, y_left, c, 1, IN_LEFT + 1)
        g_copy(n, y_left, c, 1, 9, LEFT + 1, c=other).start()
        rows_wait(n, y_right, c, 0, IN_RIGHT)
        g_copy(n, y_right, c, 0, 10, RIGHT, c=other).start()

    def rows_third(n):
        for q in (0, 1):
            rows_wait(n, y_far, c, q, IN_FAR + q)
            g_copy(n, y_far, c, q, 12 + q, FAR + q, c=other).start()

    def rows_sent(n):
        for s in range(14):
            g_copy(n, y, c, 0, s, 0, c=other).wait_send()

    def group(g):
        return (y, y_right) if g == 0 else (y_left, y_far)

    def group_rows(n, g):
        for j, yq in enumerate(group(g)):
            for q in (0, 1):
                rows_wait(n, yq, other, q, 4 * g + 2 * j + q)
        return jnp.concatenate([rows_g[n, yq].reshape(2 * HALF, -1) for yq in group(g)], axis=0)

    def core_copy(n, yq, k):
        return remote(
            partial.at[n, yq, other], from_core.at[n, yq], c_send.at[n, k], c_recv.at[n, k], c=other
        )

    def r_copy(n, src, dst, k, **device):
        return remote(src, dst, r_send.at[n, k], r_recv.at[n, k], **device)

    def chip_sum(n, yq, at_row):
        rows = pl.ds(at_row, 16)
        return partial[n, yq, c, rows, :].astype(F32) + from_core[n, yq, rows, :].astype(F32)

    def fill_ring(n, j, q, yq, extra=None):
        for at_row in range(0, QUARTER, 16):
            total = chip_sum(n, yq, q * QUARTER + at_row)
            if extra is not None:
                total = total + extra[at_row : at_row + 16, :].astype(F32)
            to_ring[n, j, q, at_row : at_row + 16, :] = total.astype(BF16)

    def sums_far(n):
        core_copy(n, y_far, 0).wait_recv()
        fill_ring(n, 0, 0, y_far)
        r_copy(n, to_ring.at[n, 0, 0], far_in.at[n, 0], 0, y=y_right).start()
        fill_ring(n, 0, 1, y_far)
        r_copy(n, to_ring.at[n, 0, 1], far_in.at[n, 1], 1, y=y_left).start()

    def sums_left(n):
        core_copy(n, y_left, 1).wait_recv()
        fill_ring(n, 1, 0, y_left)
        r_copy(n, to_ring.at[n, 1, 0], near_in.at[n, 1, 0], 2, y=y_left).start()

    def sums_right(n):
        core_copy(n, y_right, 2).wait_recv()
        fill_ring(n, 2, 1, y_right)
        r_copy(n, to_ring.at[n, 2, 1], near_in.at[n, 0, 1], 3, y=y_right).start()

    def sums_near(n):
        r_copy(n, far_in.at[n, 0], far_in.at[n, 0], 0, y=y_right).wait_recv()
        fill_ring(n, 2, 0, y_right, far_in.at[n, 0])
        r_copy(n, to_ring.at[n, 2, 0], near_in.at[n, 0, 0], 4, y=y_right).start()
        r_copy(n, far_in.at[n, 1], far_in.at[n, 1], 1, y=y_right).wait_recv()
        fill_ring(n, 1, 1, y_left, far_in.at[n, 1])
        r_copy(n, to_ring.at[n, 1, 1], near_in.at[n, 1, 1], 5, y=y_left).start()

    def near_wait(n, side, q):
        k = ((4, 3), (2, 5))[side][q]
        ref = near_in.at[n, side, q]
        r_copy(n, ref, ref, k, y=y_right).wait_recv()

    def sums_sent(n):
        for k in range(4):
            core_copy(n, y, k).wait_send()
        for k in range(6):
            r_copy(n, to_ring.at[n, 0, 0], to_ring.at[n, 0, 0], k, y=y_right).wait_send()

    def sums_wait(n):
        core_copy(n, y, 3).wait_recv()
        for side in (0, 1):
            for q in (0, 1):
                near_wait(n, side, q)

    def own_sum(n, q, at_row):
        total = chip_sum(n, y, q * QUARTER + at_row)
        for side in (0, 1):
            total = total + near_in[n, side, q, at_row : at_row + 16, :].astype(F32)
        return total

    def first_norm(h):
        for q in (0, 1):
            for at_row in range(0, QUARTER, 16):
                here = h * HALF + q * QUARTER + at_row
                wide = resid[here : here + 16, :].astype(F32)
                rows_g[h, y, c, q, at_row : at_row + 16, :] = rms_rows(wide, mix_gain[...])

    def gate_map():
        gate_w[...] = jnp.zeros_like(gate_w)
        for n in range(recur_w.shape[0]):
            block = slice(n * GATE_BLOCK, (n + 1) * GATE_BLOCK)
            gate_w[block, block] = recur_w[n]
            block_two = slice(256 + n * GATE_BLOCK, 256 + (n + 1) * GATE_BLOCK)
            gate_w[block, block_two] = input_w[n]

    def turn_up():
        own_copy(5).wait()
        own_copy(6).wait()
        for b in range(11):
            if b < 5:
                tile = gate_in[b * 128 : (b + 1) * 128, :]
            elif b < 10:
                tile = value_in[(b - 5) * 128 : (b - 4) * 128, :]
            else:
                tile = jnp.concatenate([gate_in[640:704, :], value_in[640:704, :]], axis=0)
            up_g[z, x, :, b * 128 : (b + 1) * 128] = tile.astype(F32).T.astype(BF16)

    def recur(h, g):
        w = in_g[...].reshape(-1, 256)
        proj[...] = jnp.dot(group_rows(h, g), w, preferred_element_type=F32)
        taps = conv_taps[...]
        blocks = [(j, s) for j in range(2) for s in range(2)]
        for j, s in blocks:
            yq = group(g)[j]
            rows = slice((2 * j + s) * HALF, (2 * j + s + 1) * HALF)
            wide = proj[rows, :].astype(BF16).astype(F32)
            before = jnp.zeros((8, 256), F32) if h == 0 else conv_tail[yq, s]
            if h == 0:
                conv_tail[yq, s] = wide[HALF - 8 :]
            extended = jnp.concatenate([before, wide], axis=0)
            conv = behind(extended, 3) * taps[0:1]
            conv = conv + behind(extended, 2) * taps[1:2]
            conv = conv + behind(extended, 1) * taps[2:3]
            proj[rows, :] = conv + wide * taps[3:4]
        gates[...] = jnp.dot(proj[...].astype(BF16), gate_w[...], preferred_element_type=F32)
        for j, s in blocks:
            yq = group(g)[j]
            rows = slice((2 * j + s) * HALF, (2 * j + s + 1) * HALF)
            for b in range(2):
                lanes = slice(b * 128, (b + 1) * 128)
                lanes2 = slice(256 + b * 128, 256 + (b + 1) * 128)
                rgate = jax.nn.sigmoid(gates[rows, lanes])
                igate = jax.nn.sigmoid(gates[rows, lanes2])
                a = 8.0 * rgate * decay_rate[:, lanes]
                decay = jnp.exp(-a)
                a2 = a * a
                series = 1.0 + a2 * (1.0 / 6) * (1.0 + a2 * (1.0 / 20) * (1.0 + a2 * (1.0 / 42)))
                left_over = jnp.where(a < 0.3, 2.0 * decay * (a * series), 1.0 - decay * decay)
                state = jnp.sqrt(left_over) * (igate * proj[rows, lanes])
                pos = lax.broadcasted_iota(jnp.int32, state.shape, 0)
                if h == 1:
                    state = state + jnp.where(pos == 0, decay * carry[yq, s, 0:1, lanes], 0.0)
                by = 1
                while by < HALF:
                    state = decay * shifted(state, pos, by, 0.0) + state
                    if 2 * by < HALF:
                        decay = decay * shifted(decay, pos, by, 1.0)
                    by *= 2
                if h == 0:
                    carry[yq, s, 0:1, lanes] = state[HALF - 1 :]
                recurred[h, yq, s * HALF : (s + 1) * HALF, lanes] = state.astype(BF16)

    def product(n, g, left, table, order):
        rows = jnp.concatenate([left[n % 2, yq] for yq in group(g)], axis=0)
        for zq in range(RING):
            w = jnp.concatenate([table[zq, xq] for xq in range(RING)], axis=1)
            term = jnp.dot(rows, w, preferred_element_type=F32).astype(BF16)
            for j, yq in enumerate(group(g)):
                for s in range(2):
                    lo = (2 * j + s) * HALF
                    partial[n, yq, s, :, zq * 512 : (zq + 1) * 512] = term[lo : lo + HALF]
        for j, k in order:
            core_copy(n, group(g)[j], k).start()

    def products(n, left, table):
        product(n, 1, left, table, ((1, 0), (0, 1)))
        sums_far(n)
        product(n, 0, left, table, ((1, 2), (0, 3)))
        sums_left(n)
        sums_right(n)

    def mixed(h):
        products(h, recurred, out_g)

    def lowered(h):
        products(2 + h, hidden, down_g)

    def second_norm(h):
        sums_wait(h)
        for q in (0, 1):
            for at_row in range(0, QUARTER, 16):
                lo = h * HALF + q * QUARTER + at_row
                here = slice(lo, lo + 16)
                mid = (resid[here, :].astype(F32) + own_sum(h, q, at_row)).astype(BF16)
                middle[here, :] = mid
                out = rms_rows(mid.astype(F32), mlp_gain[...])
                rows_g[2 + h, y, c, q, at_row : at_row + 16, :] = out
        rows_send(2 + h)

    def gated(extended, value, taps):
        conv = behind(extended, 2) * taps[0:1]
        conv = conv + behind(extended, 1) * taps[1:2]
        conv = conv + extended[8:] * taps[2:3]
        return (conv / (1.0 + jnp.exp(-conv)) * value).astype(BF16)

    def feed(h, g):
        w = up_g[...].reshape(-1, 1408)
        pre[...] = jnp.dot(group_rows(2 + h, g), w, preferred_element_type=F32)
        for j in range(2):
            yq = group(g)[j]
            for s in range(2):
                rows = slice((2 * j + s) * HALF, (2 * j + s + 1) * HALF)
                out = slice(s * HALF, (s + 1) * HALF)
                for b in range(6):
                    lanes = slice(b * 128, (b + 1) * 128)
                    if b < 5:
                        gate = pre[rows, lanes].astype(BF16).astype(F32)
                        value = pre[rows, 640 + b * 128 : 640 + (b + 1) * 128]
                        value = value.astype(BF16).astype(F32)
                        taps = ffn_taps[:, lanes]
                    else:
                        gate = pre[rows, 1280:1408].astype(BF16).astype(F32)
                        value = pltpu.roll(gate, 64, axis=1)
                        taps = jnp.concatenate([ffn_taps[:, 640:704], jnp.zeros((3, 64), F32)], axis=1)
                    before = jnp.zeros((8, 128), F32) if h == 0 else gate_tail[yq, s, :, lanes]
                    if h == 0:
                        gate_tail[yq, s, :, lanes] = gate[HALF - 8 :]
                    unit = gated(jnp.concatenate([before, gate], axis=0), value, taps)
                    if b < 5:
                        hidden[h, yq, out, lanes] = unit
                    else:
                        hidden[h, yq, out, 640:704] = unit[:, :64]

    def finish(h):
        sums_wait(2 + h)
        for q in (0, 1):
            for at_row in range(0, QUARTER, 16):
                lo = h * HALF + q * QUARTER + at_row
                here = slice(lo, lo + 16)
                total = middle[here, :].astype(F32) + own_sum(2 + h, q, at_row)
                result[here, :] = total.astype(BF16)

    first_send(0)
    first_send(1)
    own_copy(4).wait()
    first_norm(0)
    rows_send(0)
    turn_up()
    first_send(2)
    gate_map()
    first_norm(1)
    first_forward(0)
    first_forward(1)
    rows_first(0)
    rows_send(1)
    second_send(0)
    second_send(1)
    first_send(3)
    rows_second(0)
    first_forward(2)
    second_forward(0)
    second_forward(1)
    rows_third(0)
    second_send(2)
    weights_done(0)
    recur(0, 0)
    recur(0, 1)
    rows_first(1)
    weights_done(1)
    mixed(0)
    rows_second(1)
    first_forward(3)
    rows_third(1)
    recur(1, 0)
    recur(1, 1)
    sums_near(0)
    mixed(1)
    second_send(3)
    second_norm(0)
    sums_near(1)
    second_forward(2)
    rows_first(2)
    rows_second(2)
    second_norm(1)
    rows_third(2)
    weights_done(2)
    feed(0, 0)
    feed(0, 1)
    rows_first(3)
    second_forward(3)
    rows_second(3)
    weights_done(3)
    lowered(0)
    rows_third(3)
    feed(1, 0)
    feed(1, 1)
    sums_near(2)
    lowered(1)
    finish(0)
    sums_near(3)
    finish(1)

    for n in range(4):
        rows_sent(n)
        sums_sent(n)
    for i in range(4):
        weights_sent(i)


def shards(
    resid,
    mix_gain,
    in_weight,
    conv_taps,
    recur_gate_w,
    input_gate_w,
    decay_rate,
    out_weight,
    mlp_gain,
    up_gate_w,
    up_val_w,
    ffn_taps,
    down_weight,
):
    vmem = pl.BlockSpec(memory_space=pltpu.VMEM)
    hbm = pl.BlockSpec(memory_space=pl.ANY)
    dma = pltpu.SemaphoreType.DMA
    width = resid.shape[1]
    units = up_gate_w.shape[1]
    return pl.pallas_call(
        kernel,
        name="layer",
        out_shape=jax.ShapeDtypeStruct(resid.shape, BF16),
        in_specs=[hbm, vmem, hbm, vmem, vmem, vmem, vmem, hbm, vmem, hbm, hbm, vmem, hbm],
        out_specs=vmem,
        scratch_shapes=[
            pltpu.VMEM(resid.shape, BF16),
            pltpu.VMEM((units, 128), BF16),
            pltpu.VMEM((units, 128), BF16),
            pltpu.VMEM((RING, RING, *in_weight.shape), BF16),
            pltpu.VMEM((RING, RING, *out_weight.shape), BF16),
            pltpu.VMEM((RING, RING, up_gate_w.shape[0], 2 * units), BF16),
            pltpu.VMEM((RING, RING, *down_weight.shape), BF16),
            pltpu.VMEM((4, RING, 2, 2, QUARTER, width), BF16),
            pltpu.VMEM((256, 512), BF16),
            pltpu.VMEM((4 * HALF, 256), F32),
            pltpu.VMEM((4 * HALF, 512), F32),
            pltpu.VMEM((RING, 2, 8, 256), F32),
            pltpu.VMEM((RING, 2, 8, 256), F32),
            pltpu.VMEM((2, RING, 2 * HALF, 256), BF16),
            pltpu.VMEM((4 * HALF, 2 * units), F32),
            pltpu.VMEM((RING, 2, 8, 768), F32),
            pltpu.VMEM((2, RING, 2 * HALF, units), BF16),
            pltpu.VMEM((4, RING, 2, HALF, width), BF16),
            pltpu.VMEM((4, RING, HALF, width), BF16),
            pltpu.VMEM((4, 3, 2, QUARTER, width), BF16),
            pltpu.VMEM((4, 2, QUARTER, width), BF16),
            pltpu.VMEM((4, 2, 2, QUARTER, width), BF16),
            pltpu.VMEM((SEQ, width), BF16),
            dma((4, 4, 6)),
            dma((4, 4, 6)),
            dma((7,)),
            dma((4, 14)),
            dma((4, 14)),
            dma((4, 4)),
            dma((4, 4)),
            dma((4, 6)),
            dma((4, 6)),
        ],
        compiler_params=pltpu.CompilerParams(
            collective_id=0, has_side_effects=True, vmem_limit_bytes=60 * 1024 * 1024
        ),
    )(
        resid,
        mix_gain[None],
        in_weight,
        conv_taps,
        recur_gate_w,
        input_gate_w,
        decay_rate[None],
        out_weight,
        mlp_gain[None],
        up_gate_w.T,
        up_val_w.T,
        ffn_taps,
        down_weight,
    )


def solution(mesh):
    split = Mesh(mesh.devices.reshape(RING, RING, RING, 2), ("z", "x", "y", "c"))
    fs, tp = ("z", "x"), ("y", "c")
    rows = ("z", "x", "y", "c")
    return jax.shard_map(
        shards,
        mesh=split,
        in_specs=(
            P(rows, None),
            P(),
            P(fs, tp),
            P(None, tp),
            P(tp, None, None),
            P(tp, None, None),
            P(tp),
            P(tp, fs),
            P(),
            P(fs, tp),
            P(fs, tp),
            P(None, tp),
            P(tp, fs),
        ),
        out_specs=P(rows, None),
        check_vma=False,
    )
```

```python
import jax
import jax.numpy as jnp
from jax import lax
from jax.experimental import pallas as pl
from jax.experimental.pallas import tpu as pltpu
from jax.sharding import Mesh
from jax.sharding import PartitionSpec as P

GATE_BLOCK = 64
SEQ = 128
HALF = 64
QUARTER = 32
RING = 4
MESH = pl.DeviceIdType.MESH
BF16 = jnp.bfloat16
F32 = jnp.float32

OWN, RIGHT, LEFT, FAR, IN_RIGHT, IN_LEFT, IN_FAR = 0, 2, 4, 6, 8, 10, 12


ORDER = (
    ("S1", 0),
    ("RS", 1),
    ("RS", 0),
    ("S1", 1),
    ("S1", 3),
    ("F1", 0, 3),
    ("F1", 0, 0),
    ("F1", 1, 0),
    ("F1", 1, 2),
    ("S1", 2),
    ("F1", 0, 1),
    ("F1", 1, 1),
    ("S2", 0, 3),
    ("F1", 1, 3),
    ("F1", 0, 2),
    ("S2", 1, 0),
    ("S2", 0, 0),
    ("S2", 1, 2),
    ("S2", 0, 2),
    ("F1", 3, 3),
    ("F1", 3, 1),
    ("F1", 2, 0),
    ("F1", 2, 2),
    ("S2", 0, 1),
    ("S2", 1, 1),
    ("F1", 2, 3),
    ("R1", 0),
    ("R2", 1),
    ("S2", 1, 3),
    ("R2", 0),
    ("F2", 0, 0),
    ("F2", 1, 0),
    ("F2", 0, 3),
    ("F2", 0, 1),
    ("F2", 0, 2),
    ("F2", 1, 2),
    ("R1", 1),
    ("F1", 2, 1),
    ("F2", 1, 3),
    ("S2", 3, 3),
    ("F1", 3, 0),
    ("F2", 1, 1),
    ("S2", 2, 0),
    ("R3", 0),
    ("S2", 2, 1),
    ("F1", 3, 2),
    ("D", 0),
    ("rec", 0, 1),
    ("S2", 2, 3),
    ("D", 1),
    ("S2", 2, 2),
    ("R3", 1),
    ("prod", 0, 1),
    ("rec", 0, 0),
    ("prod", 0, 0),
    ("sfar", 0),
    ("S2", 3, 1),
    ("rec", 1, 1),
    ("sright", 0),
    ("sleft", 0),
    ("prod", 1, 1),
    ("rec", 1, 0),
    ("near", 0),
    ("prod", 1, 0),
    ("sfar", 1),
    ("sleft", 1),
    ("sright", 1),
    ("F2", 2, 1),
    ("S2", 3, 0),
    ("F2", 2, 3),
    ("F2", 2, 0),
    ("S2", 3, 2),
    ("norm2", 0),
    ("near", 1),
    ("F2", 2, 2),
    ("RS", 2),
    ("R1", 2),
    ("F2", 3, 2),
    ("F2", 3, 0),
    ("norm2", 1),
    ("F2", 3, 3),
    ("F2", 3, 1),
    ("R2", 2),
    ("RS", 3),
    ("R3", 2),
    ("D", 2),
    ("feed", 0, 0),
    ("R1", 3),
    ("feed", 0, 1),
    ("D", 3),
    ("prod", 2, 1),
    ("prod", 2, 0),
    ("sfar", 2),
    ("R3", 3),
    ("R2", 3),
    ("sleft", 2),
    ("sright", 2),
    ("feed", 1, 1),
    ("prod", 3, 1),
    ("near", 2),
    ("feed", 1, 0),
    ("sfar", 3),
    ("prod", 3, 0),
    ("sright", 3),
    ("sleft", 3),
    ("sent",),
    ("near", 3),
    ("fin", 0),
    ("fin", 1),
)
WAITED = {0: 3, 1: 0, 3: 3}


def remote(src, dst, send_sem, recv_sem, **device):
    return pltpu.make_async_remote_copy(
        src_ref=src,
        dst_ref=dst,
        send_sem=send_sem,
        recv_sem=recv_sem,
        device_id=device,
        device_id_type=MESH,
    )


def rms_rows(wide, gain):
    scale = lax.rsqrt(jnp.mean(wide * wide, axis=-1, keepdims=True) + 1e-06)
    return (wide * scale * gain).astype(BF16)


def shifted(values, rows, by, fill):
    return jnp.where(rows >= by, pltpu.roll(values, by, axis=0), fill)


def behind(extended, by):
    return pltpu.roll(extended, by, axis=0)[8:]


def kernel(
    resid_hbm,
    mix_gain_hbm,
    in_w,
    conv_taps_hbm,
    recur_w_hbm,
    input_w_hbm,
    decay_rate_hbm,
    out_w,
    mlp_gain_hbm,
    gate_t,
    value_t,
    ffn_taps_hbm,
    down_w,
    result_hbm,
    resid,
    gate_in,
    value_in,
    mix_gain,
    conv_taps,
    recur_w,
    input_w,
    decay_rate,
    mlp_gain,
    ffn_taps,
    result,
    in_g,
    out_g,
    up_g,
    down_g,
    rows_g,
    gate_w,
    proj,
    gates,
    conv_tail,
    carry,
    recurred,
    pre,
    gate_tail,
    hidden,
    partial,
    from_core,
    to_ring,
    far_in,
    near_in,
    middle,
    w_send,
    w_recv,
    l_sem,
    g_send,
    g_recv,
    c_send,
    c_recv,
    r_send,
    r_recv,
):
    z, x, y, c = (lax.axis_index(a) for a in ("z", "x", "y", "c"))
    at = {"z": z, "x": x, "y": y}

    def nxt(axis, by):
        return lax.rem(at[axis] + (by + RING), RING)

    other = 1 - c
    y_right, y_left, y_far = nxt("y", 1), nxt("y", -1), nxt("y", 2)

    weights = ((in_w, in_g), (out_w, out_g), (None, up_g), (down_w, down_g))

    def own_copy(i):
        if i < 4:
            src, g = weights[i]
            return pltpu.make_async_copy(src, g.at[z, x], l_sem.at[i])
        src, dst = (
            (resid_hbm, resid),
            (gate_t, gate_in),
            (value_t, value_in),
            (mix_gain_hbm, mix_gain),
            (recur_w_hbm, recur_w),
            (input_w_hbm, input_w),
            (conv_taps_hbm, conv_taps),
            (decay_rate_hbm, decay_rate),
            (mlp_gain_hbm, mlp_gain),
            (ffn_taps_hbm, ffn_taps),
        )[i - 4]
        return pltpu.make_async_copy(src, dst, l_sem.at[i])

    def result_copy(h):
        here = pl.ds(h * HALF, HALF)
        return pltpu.make_async_copy(result.at[here], result_hbm.at[here], l_sem.at[14 + h])

    for i in (4, 7, 5, 6, 8, 9, 10, 11, 12, 13, 0, 1, 3):
        own_copy(i).start()

    barrier = pltpu.get_barrier_semaphore()
    for axis in ("z", "x", "y"):
        for by in (1, -1):
            pl.semaphore_signal(
                barrier, inc=1, device_id={axis: nxt(axis, by)}, device_id_type=MESH
            )
    pl.semaphore_signal(barrier, inc=1, device_id={"c": other}, device_id_type=MESH)

    def piece(i, p):
        rows = weights[i][1].shape[2] // 4
        return pl.ds(p * rows, rows)

    def axes_of(p):
        return ("x", "z") if p < 2 else ("z", "x")

    def slot(i, p, axis, by):
        g = weights[i][1]
        if axis == "x":
            return g.at[z, nxt("x", by), piece(i, p)]
        return g.at[nxt("z", by), x, piece(i, p)]

    def line(i, p, axis, by):
        g = weights[i][1]
        if axis == "z":
            return g.at[nxt("z", by), :, piece(i, p)]
        return g.at[:, nxt("x", by), piece(i, p)]

    def w_copy(i, p, src, dst, k, axis, by):
        return remote(src, dst, w_send.at[i, p, k], w_recv.at[i, p, k], **{axis: nxt(axis, by)})

    def first_send(i):
        src = weights[i][0]
        for p in range(4):
            axis = axes_of(p)[0]
            here = slot(i, p, axis, 0)
            for k, by in ((0, 1), (1, -1)):
                w_copy(i, p, here if src is None else src.at[piece(i, p)], here, k, axis, by).start()

    def first_wait(i, p, k):
        axis = axes_of(p)[0]
        there = slot(i, p, axis, (-1, 1, 2)[k])
        w_copy(i, p, there, there, k, axis, 1).wait_recv()

    def first_forward(i, p):
        axis = axes_of(p)[0]
        k = p % 2
        first_wait(i, p, k)
        by = 1 if k == 0 else -1
        there = slot(i, p, axis, -by)
        w_copy(i, p, there, there, 2, axis, by).start()

    def second_send(i, p):
        if p == WAITED.get(i):
            own_copy(i).wait()
        axis = axes_of(p)[1]
        first_wait(i, p, 1 - p % 2)
        first_wait(i, p, 2)
        here = line(i, p, axis, 0)
        for k, by in ((3, 1), (4, -1)):
            w_copy(i, p, here, here, k, axis, by).start()

    def second_wait(i, p, k):
        axis = axes_of(p)[1]
        there = line(i, p, axis, (-1, 1, 2)[k - 3])
        w_copy(i, p, there, there, k, axis, 1).wait_recv()

    def second_forward(i, p):
        axis = axes_of(p)[1]
        k = 3 + p % 2
        second_wait(i, p, k)
        by = 1 if k == 3 else -1
        there = line(i, p, axis, -by)
        w_copy(i, p, there, there, 5, axis, by).start()

    def weights_done(i):
        for p in range(4):
            second_wait(i, p, 4 - p % 2)
            second_wait(i, p, 5)

    def weights_sent(i):
        for p in range(4):
            first, second = axes_of(p)
            one, four = slot(i, p, first, 0), line(i, p, second, 0)
            for k in range(6):
                ref = one if k < 3 else four
                w_copy(i, p, ref, ref, k, first, 1).wait_send()

    def g_copy(n, yq, cq, q, s, r, **device):
        ref = rows_g.at[n, yq, cq, q]
        return remote(ref, ref, g_send.at[n, s], g_recv.at[n, r], **device)

    def rows_wait(n, yq, cq, q, r):
        g_copy(n, yq, cq, q, 0, r, c=other).wait_recv()

    def rows_send(n):
        for q in (0, 1):
            g_copy(n, y, c, q, q, IN_LEFT + q, y=y_right).start()
            g_copy(n, y, c, 1 - q, 2 + 1 - q, IN_RIGHT + 1 - q, y=y_left).start()
            g_copy(n, y, c, q, 4 + q, OWN + q, c=other).start()

    def rows_first(n):
        rows_wait(n, y_left, c, 0, IN_LEFT)
        g_copy(n, y_left, c, 0, 6, IN_FAR, y=y_right).start()
        g_copy(n, y_left, c, 0, 8, LEFT, c=other).start()
        rows_wait(n, y_right, c, 1, IN_RIGHT + 1)
        g_copy(n, y_right, c, 1, 7, IN_FAR + 1, y=y_left).start()
        g_copy(n, y_right, c, 1, 11, RIGHT + 1, c=other).start()

    def rows_second(n):
        rows_wait(n, y_left, c, 1, IN_LEFT + 1)
        g_copy(n, y_left, c, 1, 9, LEFT + 1, c=other).start()
        rows_wait(n, y_right, c, 0, IN_RIGHT)
        g_copy(n, y_right, c, 0, 10, RIGHT, c=other).start()

    def rows_third(n):
        for q in (0, 1):
            rows_wait(n, y_far, c, q, IN_FAR + q)
            g_copy(n, y_far, c, q, 12 + q, FAR + q, c=other).start()

    def rows_sent(n):
        for s in range(14):
            g_copy(n, y, c, 0, s, 0, c=other).wait_send()

    def group(g):
        return (y, y_right) if g == 0 else (y_left, y_far)

    def group_rows(n, g):
        for j, yq in enumerate(group(g)):
            for q in (0, 1):
                rows_wait(n, yq, other, q, 4 * g + 2 * j + q)
        return jnp.concatenate([rows_g[n, yq].reshape(2 * HALF, -1) for yq in group(g)], axis=0)

    def core_copy(n, yq, k):
        return remote(
            partial.at[n, yq, other], from_core.at[n, yq], c_send.at[n, k], c_recv.at[n, k], c=other
        )

    def r_copy(n, src, dst, k, **device):
        return remote(src, dst, r_send.at[n, k], r_recv.at[n, k], **device)

    def chip_sum(n, yq, at_row):
        rows = pl.ds(at_row, 16)
        return partial[n, yq, c, rows, :].astype(F32) + from_core[n, yq, rows, :].astype(F32)

    def fill_ring(n, j, q, yq, extra=None):
        for at_row in range(0, QUARTER, 16):
            total = chip_sum(n, yq, q * QUARTER + at_row)
            if extra is not None:
                total = total + extra[at_row : at_row + 16, :].astype(F32)
            to_ring[n, j, q, at_row : at_row + 16, :] = total.astype(BF16)

    def sums_far(n):
        core_copy(n, y_far, 0).wait_recv()
        fill_ring(n, 0, 0, y_far)
        r_copy(n, to_ring.at[n, 0, 0], far_in.at[n, 0], 0, y=y_right).start()
        fill_ring(n, 0, 1, y_far)
        r_copy(n, to_ring.at[n, 0, 1], far_in.at[n, 1], 1, y=y_left).start()

    def sums_left(n):
        core_copy(n, y_left, 1).wait_recv()
        fill_ring(n, 1, 0, y_left)
        r_copy(n, to_ring.at[n, 1, 0], near_in.at[n, 1, 0], 2, y=y_left).start()

    def sums_right(n):
        core_copy(n, y_right, 2).wait_recv()
        fill_ring(n, 2, 1, y_right)
        r_copy(n, to_ring.at[n, 2, 1], near_in.at[n, 0, 1], 3, y=y_right).start()

    def sums_near(n):
        r_copy(n, far_in.at[n, 0], far_in.at[n, 0], 0, y=y_right).wait_recv()
        fill_ring(n, 2, 0, y_right, far_in.at[n, 0])
        r_copy(n, to_ring.at[n, 2, 0], near_in.at[n, 0, 0], 4, y=y_right).start()
        r_copy(n, far_in.at[n, 1], far_in.at[n, 1], 1, y=y_right).wait_recv()
        fill_ring(n, 1, 1, y_left, far_in.at[n, 1])
        r_copy(n, to_ring.at[n, 1, 1], near_in.at[n, 1, 1], 5, y=y_left).start()

    def near_wait(n, side, q):
        k = ((4, 3), (2, 5))[side][q]
        ref = near_in.at[n, side, q]
        r_copy(n, ref, ref, k, y=y_right).wait_recv()

    def sums_sent(n):
        for k in range(4):
            core_copy(n, y, k).wait_send()
        for k in range(6):
            r_copy(n, to_ring.at[n, 0, 0], to_ring.at[n, 0, 0], k, y=y_right).wait_send()

    def sums_wait(n):
        core_copy(n, y, 3).wait_recv()
        for side in (0, 1):
            for q in (0, 1):
                near_wait(n, side, q)

    def own_sum(n, q, at_row):
        total = chip_sum(n, y, q * QUARTER + at_row)
        for side in (0, 1):
            total = total + near_in[n, side, q, at_row : at_row + 16, :].astype(F32)
        return total

    def first_norm(h):
        for q in (0, 1):
            for at_row in range(0, QUARTER, 16):
                here = h * HALF + q * QUARTER + at_row
                wide = resid[here : here + 16, :].astype(F32)
                rows_g[h, y, c, q, at_row : at_row + 16, :] = rms_rows(wide, mix_gain[...])

    def gate_map():
        gate_w[...] = jnp.zeros_like(gate_w)
        for n in range(recur_w.shape[0]):
            block = slice(n * GATE_BLOCK, (n + 1) * GATE_BLOCK)
            gate_w[block, block] = recur_w[n]
            block_two = slice(256 + n * GATE_BLOCK, 256 + (n + 1) * GATE_BLOCK)
            gate_w[block, block_two] = input_w[n]

    def turn_up():
        for b in range(11):
            if b < 5:
                tile = gate_in[b * 128 : (b + 1) * 128, :]
            elif b < 10:
                tile = value_in[(b - 5) * 128 : (b - 4) * 128, :]
            else:
                tile = jnp.concatenate([gate_in[640:704, :], value_in[640:704, :]], axis=0)
            up_g[z, x, :, b * 128 : (b + 1) * 128] = tile.astype(F32).T.astype(BF16)

    def recur(h, g):
        w = in_g[...].reshape(-1, 256)
        proj[...] = jnp.dot(group_rows(h, g), w, preferred_element_type=F32)
        taps = conv_taps[...]
        blocks = [(j, s) for j in range(2) for s in range(2)]
        for j, s in blocks:
            yq = group(g)[j]
            rows = slice((2 * j + s) * HALF, (2 * j + s + 1) * HALF)
            wide = proj[rows, :].astype(BF16).astype(F32)
            before = jnp.zeros((8, 256), F32) if h == 0 else conv_tail[yq, s]
            if h == 0:
                conv_tail[yq, s] = wide[HALF - 8 :]
            extended = jnp.concatenate([before, wide], axis=0)
            conv = behind(extended, 3) * taps[0:1]
            conv = conv + behind(extended, 2) * taps[1:2]
            conv = conv + behind(extended, 1) * taps[2:3]
            proj[rows, :] = conv + wide * taps[3:4]
        gates[...] = jnp.dot(proj[...].astype(BF16), gate_w[...], preferred_element_type=F32)
        for j, s in blocks:
            yq = group(g)[j]
            rows = slice((2 * j + s) * HALF, (2 * j + s + 1) * HALF)
            for b in range(2):
                lanes = slice(b * 128, (b + 1) * 128)
                lanes2 = slice(256 + b * 128, 256 + (b + 1) * 128)
                rgate = jax.nn.sigmoid(gates[rows, lanes])
                igate = jax.nn.sigmoid(gates[rows, lanes2])
                a = 8.0 * rgate * decay_rate[:, lanes]
                decay = jnp.exp(-a)
                a2 = a * a
                series = 1.0 + a2 * (1.0 / 6) * (1.0 + a2 * (1.0 / 20) * (1.0 + a2 * (1.0 / 42)))
                left_over = jnp.where(a < 0.3, 2.0 * decay * (a * series), 1.0 - decay * decay)
                state = jnp.sqrt(left_over) * (igate * proj[rows, lanes])
                pos = lax.broadcasted_iota(jnp.int32, state.shape, 0)
                if h == 1:
                    state = state + jnp.where(pos == 0, decay * carry[yq, s, 0:1, lanes], 0.0)
                by = 1
                while by < HALF:
                    state = decay * shifted(state, pos, by, 0.0) + state
                    if 2 * by < HALF:
                        decay = decay * shifted(decay, pos, by, 1.0)
                    by *= 2
                if h == 0:
                    carry[yq, s, 0:1, lanes] = state[HALF - 1 :]
                recurred[h, yq, s * HALF : (s + 1) * HALF, lanes] = state.astype(BF16)

    def product(n, g, left, table, order):
        rows = jnp.concatenate([left[n % 2, yq] for yq in group(g)], axis=0)
        for zq in range(RING):
            w = jnp.concatenate([table[zq, xq] for xq in range(RING)], axis=1)
            term = jnp.dot(rows, w, preferred_element_type=F32).astype(BF16)
            for j, yq in enumerate(group(g)):
                for s in range(2):
                    lo = (2 * j + s) * HALF
                    partial[n, yq, s, :, zq * 512 : (zq + 1) * 512] = term[lo : lo + HALF]
        for j, k in order:
            core_copy(n, group(g)[j], k).start()

    def step_product(n, g):
        order = ((1, 2), (0, 3)) if g == 0 else ((1, 0), (0, 1))
        if n < 2:
            product(n, g, recurred, out_g, order)
        else:
            product(n, g, hidden, down_g, order)

    def second_norm(h):
        sums_wait(h)
        for q in (0, 1):
            for at_row in range(0, QUARTER, 16):
                lo = h * HALF + q * QUARTER + at_row
                here = slice(lo, lo + 16)
                mid = (resid[here, :].astype(F32) + own_sum(h, q, at_row)).astype(BF16)
                middle[here, :] = mid
                out = rms_rows(mid.astype(F32), mlp_gain[...])
                rows_g[2 + h, y, c, q, at_row : at_row + 16, :] = out

    def gated(extended, value, taps):
        conv = behind(extended, 2) * taps[0:1]
        conv = conv + behind(extended, 1) * taps[1:2]
        conv = conv + extended[8:] * taps[2:3]
        return (conv / (1.0 + jnp.exp(-conv)) * value).astype(BF16)

    def feed(h, g):
        w = up_g[...].reshape(-1, 1408)
        pre[...] = jnp.dot(group_rows(2 + h, g), w, preferred_element_type=F32)
        for j in range(2):
            yq = group(g)[j]
            for s in range(2):
                rows = slice((2 * j + s) * HALF, (2 * j + s + 1) * HALF)
                out = slice(s * HALF, (s + 1) * HALF)
                for b in range(6):
                    lanes = slice(b * 128, (b + 1) * 128)
                    if b < 5:
                        gate = pre[rows, lanes].astype(BF16).astype(F32)
                        value = pre[rows, 640 + b * 128 : 640 + (b + 1) * 128]
                        value = value.astype(BF16).astype(F32)
                        taps = ffn_taps[:, lanes]
                    else:
                        gate = pre[rows, 1280:1408].astype(BF16).astype(F32)
                        value = pltpu.roll(gate, 64, axis=1)
                        taps = jnp.concatenate([ffn_taps[:, 640:704], jnp.zeros((3, 64), F32)], axis=1)
                    before = jnp.zeros((8, 128), F32) if h == 0 else gate_tail[yq, s, :, lanes]
                    if h == 0:
                        gate_tail[yq, s, :, lanes] = gate[HALF - 8 :]
                    unit = gated(jnp.concatenate([before, gate], axis=0), value, taps)
                    if b < 5:
                        hidden[h, yq, out, lanes] = unit
                    else:
                        hidden[h, yq, out, 640:704] = unit[:, :64]

    def finish(h):
        sums_wait(2 + h)
        for q in (0, 1):
            for at_row in range(0, QUARTER, 16):
                lo = h * HALF + q * QUARTER + at_row
                here = slice(lo, lo + 16)
                total = middle[here, :].astype(F32) + own_sum(2 + h, q, at_row)
                result[here, :] = total.astype(BF16)
        result_copy(h).start()

    own_copy(4).wait()
    own_copy(7).wait()
    first_norm(0)
    own_copy(5).wait()
    own_copy(6).wait()
    turn_up()
    own_copy(8).wait()
    own_copy(9).wait()
    gate_map()
    first_norm(1)
    for i in (10, 11, 12, 13):
        own_copy(i).wait()
    pl.semaphore_wait(barrier, 7)

    def sent():
        for n in range(4):
            rows_sent(n)
            if n < 3:
                sums_sent(n)
        for i in range(4):
            weights_sent(i)

    steps = {
        "S1": first_send,
        "F1": first_forward,
        "S2": second_send,
        "F2": second_forward,
        "D": weights_done,
        "RS": rows_send,
        "R1": rows_first,
        "R2": rows_second,
        "R3": rows_third,
        "rec": recur,
        "feed": feed,
        "prod": step_product,
        "sfar": sums_far,
        "sleft": sums_left,
        "sright": sums_right,
        "near": sums_near,
        "norm2": second_norm,
        "fin": finish,
        "sent": sent,
    }
    for name, *where in ORDER:
        steps[name](*where)
    sums_sent(3)
    result_copy(0).wait()
    result_copy(1).wait()


def shards(
    resid,
    mix_gain,
    in_weight,
    conv_taps,
    recur_gate_w,
    input_gate_w,
    decay_rate,
    out_weight,
    mlp_gain,
    up_gate_w,
    up_val_w,
    ffn_taps,
    down_weight,
):
    hbm = pl.BlockSpec(memory_space=pl.ANY)
    dma = pltpu.SemaphoreType.DMA
    width = resid.shape[1]
    units = up_gate_w.shape[1]
    return pl.pallas_call(
        kernel,
        name="layer",
        out_shape=pltpu.VMEM(resid.shape, BF16),
        in_specs=[hbm] * 13,
        out_specs=pl.BlockSpec(memory_space=pltpu.VMEM),
        scratch_shapes=[
            pltpu.VMEM(resid.shape, BF16),
            pltpu.VMEM((units, 128), BF16),
            pltpu.VMEM((units, 128), BF16),
            pltpu.VMEM((1, width), F32),
            pltpu.VMEM(conv_taps.shape, F32),
            pltpu.VMEM(recur_gate_w.shape, BF16),
            pltpu.VMEM(input_gate_w.shape, BF16),
            pltpu.VMEM((1, *decay_rate.shape), F32),
            pltpu.VMEM((1, width), F32),
            pltpu.VMEM(ffn_taps.shape, F32),
            pltpu.VMEM(resid.shape, BF16),
            pltpu.VMEM((RING, RING, *in_weight.shape), BF16),
            pltpu.VMEM((RING, RING, *out_weight.shape), BF16),
            pltpu.VMEM((RING, RING, up_gate_w.shape[0], 2 * units), BF16),
            pltpu.VMEM((RING, RING, *down_weight.shape), BF16),
            pltpu.VMEM((4, RING, 2, 2, QUARTER, width), BF16),
            pltpu.VMEM((256, 512), BF16),
            pltpu.VMEM((4 * HALF, 256), F32),
            pltpu.VMEM((4 * HALF, 512), F32),
            pltpu.VMEM((RING, 2, 8, 256), F32),
            pltpu.VMEM((RING, 2, 8, 256), F32),
            pltpu.VMEM((2, RING, 2 * HALF, 256), BF16),
            pltpu.VMEM((4 * HALF, 2 * units), F32),
            pltpu.VMEM((RING, 2, 8, 768), F32),
            pltpu.VMEM((2, RING, 2 * HALF, units), BF16),
            pltpu.VMEM((4, RING, 2, HALF, width), BF16),
            pltpu.VMEM((4, RING, HALF, width), BF16),
            pltpu.VMEM((4, 3, 2, QUARTER, width), BF16),
            pltpu.VMEM((4, 2, QUARTER, width), BF16),
            pltpu.VMEM((4, 2, 2, QUARTER, width), BF16),
            pltpu.VMEM((SEQ, width), BF16),
            dma((4, 4, 6)),
            dma((4, 4, 6)),
            dma((16,)),
            dma((4, 14)),
            dma((4, 14)),
            dma((4, 4)),
            dma((4, 4)),
            dma((4, 6)),
            dma((4, 6)),
        ],
        compiler_params=pltpu.CompilerParams(
            collective_id=0, has_side_effects=True, vmem_limit_bytes=56 * 1024 * 1024
        ),
    )(
        resid,
        mix_gain[None],
        in_weight,
        conv_taps,
        recur_gate_w,
        input_gate_w,
        decay_rate[None],
        out_weight,
        mlp_gain[None],
        up_gate_w.T,
        up_val_w.T,
        ffn_taps,
        down_weight,
    )


def solution(mesh):
    split = Mesh(mesh.devices.reshape(RING, RING, RING, 2), ("z", "x", "y", "c"))
    fs, tp = ("z", "x"), ("y", "c")
    rows = ("z", "x", "y", "c")
    return jax.shard_map(
        shards,
        mesh=split,
        in_specs=(
            P(rows, None),
            P(),
            P(fs, tp),
            P(None, tp),
            P(tp, None, None),
            P(tp, None, None),
            P(tp),
            P(tp, fs),
            P(),
            P(fs, tp),
            P(fs, tp),
            P(None, tp),
            P(tp, fs),
        ),
        out_specs=P(rows, None),
        check_vma=False,
    )
```

```python
import jax
import jax.numpy as jnp
from jax import lax
from jax.experimental import pallas as pl
from jax.experimental.pallas import tpu as pltpu
from jax.sharding import Mesh
from jax.sharding import PartitionSpec as P

GATE_BLOCK = 64
SEQ = 128
HALF = 64
QUARTER = 32
RING = 4
MESH = pl.DeviceIdType.MESH
BF16 = jnp.bfloat16
F32 = jnp.float32

OWN, RIGHT, LEFT, FAR, IN_RIGHT, IN_LEFT, IN_FAR = 0, 2, 4, 6, 8, 10, 12


PIECES = (4, 4, 4, 4)
X_FIRST = (2, 2, 2, 2)
SUMS = ((0, 0, 16), (1, 0, 16), (2, 0, 9), (3, 0, 9), (2, 9, 16), (3, 9, 16))
BLOCKS = tuple(
    sorted(((dz, dx) for dz in (0, 1, -1, 2) for dx in (0, 1, -1, 2)), key=lambda d: 2 in d)
)
ORDER = (
    ("S1", 0, 1),
    ("S1", 1, 0),
    ("S1", 1, 3),
    ("RS", 0),
    ("S1", 0, 3),
    ("S1", 0, 0),
    ("S1", 1, 2),
    ("S1", 0, 2),
    ("S1", 1, 1),
    ("S1", 2, 2),
    ("S1", 2, 0),
    ("F1", 1, 3),
    ("F1", 1, 0),
    ("F1", 0, 3),
    ("F1", 0, 0),
    ("S1", 2, 3),
    ("RS", 1),
    ("S1", 2, 1),
    ("S1", 3, 1),
    ("F1", 1, 2),
    ("F1", 0, 2),
    ("F1", 0, 1),
    ("F1", 2, 2),
    ("F1", 2, 0),
    ("S2", 0, 3),
    ("F1", 1, 1),
    ("S2", 1, 0),
    ("S2", 0, 0),
    ("S2", 0, 1),
    ("S2", 0, 2),
    ("S2", 1, 3),
    ("S2", 1, 2),
    ("S2", 1, 1),
    ("R1", 0),
    ("F1", 2, 3),
    ("F1", 3, 1),
    ("F2", 0, 3),
    ("R2", 1),
    ("F2", 0, 0),
    ("F2", 0, 2),
    ("F2", 0, 1),
    ("F2", 1, 1),
    ("R1", 1),
    ("F2", 1, 3),
    ("F2", 1, 0),
    ("R3", 0),
    ("F2", 1, 2),
    ("F1", 2, 1),
    ("S1", 3, 2),
    ("R2", 0),
    ("S1", 3, 0),
    ("S1", 3, 3),
    ("S2", 2, 0),
    ("S2", 2, 2),
    ("DA", 1),
    ("DA", 0),
    ("DB", 0),
    ("rec", 0, 1),
    ("R3", 1),
    ("DB", 1),
    ("prod", 0, 1),
    ("rec", 0, 0),
    ("sfar", 0),
    ("prod", 0, 0),
    ("S2", 2, 3),
    ("sleft", 0),
    ("F1", 3, 3),
    ("F1", 3, 2),
    ("sright", 0),
    ("rec", 1, 1),
    ("S2", 2, 1),
    ("prod", 1, 1),
    ("near", 0),
    ("sfar", 1),
    ("S2", 3, 2),
    ("F2", 2, 0),
    ("F1", 3, 0),
    ("S2", 3, 1),
    ("rec", 1, 0),
    ("sleft", 1),
    ("F2", 2, 2),
    ("prod", 1, 0),
    ("sright", 1),
    ("norm2", 0),
    ("near", 1),
    ("RS", 2),
    ("F2", 2, 3),
    ("F2", 2, 1),
    ("norm2", 1),
    ("S2", 3, 3),
    ("DA", 2),
    ("R1", 2),
    ("S2", 3, 0),
    ("F2", 3, 1),
    ("RS", 3),
    ("DB", 2),
    ("R2", 2),
    ("F2", 3, 2),
    ("R3", 2),
    ("feed", 0, 0),
    ("R1", 3),
    ("F2", 3, 3),
    ("F2", 3, 0),
    ("DA", 3),
    ("feed", 0, 1),
    ("R2", 3),
    ("prod", 2, 1),
    ("prod", 2, 0),
    ("sfar", 2),
    ("R3", 3),
    ("sright", 2),
    ("sleft", 2),
    ("DB", 3),
    ("prod", 4, 1),
    ("feed", 1, 1),
    ("sfar", 4),
    ("near", 2),
    ("prod", 5, 1),
    ("prod", 4, 0),
    ("prod", 3, 1),
    ("sfar", 5),
    ("sright", 4),
    ("sleft", 4),
    ("near", 4),
    ("feed", 1, 0),
    ("sfar", 3),
    ("sleft", 5),
    ("prod", 5, 0),
    ("fin", 2),
    ("sright", 5),
    ("near", 5),
    ("sleft", 3),
    ("prod", 3, 0),
    ("sright", 3),
    ("fin", 4),
    ("near", 3),
    ("sent",),
    ("fin", 5),
    ("fin", 3),
)
WAITED = {0: 3, 1: 0, 3: 2}


def remote(src, dst, send_sem, recv_sem, **device):
    return pltpu.make_async_remote_copy(
        src_ref=src,
        dst_ref=dst,
        send_sem=send_sem,
        recv_sem=recv_sem,
        device_id=device,
        device_id_type=MESH,
    )


def rms_rows(wide, gain):
    scale = lax.rsqrt(jnp.mean(wide * wide, axis=-1, keepdims=True) + 1e-06)
    return (wide * scale * gain).astype(BF16)


def shifted(values, rows, by, fill):
    return jnp.where(rows >= by, pltpu.roll(values, by, axis=0), fill)


def behind(extended, by):
    return pltpu.roll(extended, by, axis=0)[8:]


def kernel(
    resid_hbm,
    mix_gain_hbm,
    in_w,
    conv_taps_hbm,
    recur_w_hbm,
    input_w_hbm,
    decay_rate_hbm,
    out_w,
    mlp_gain_hbm,
    gate_t,
    value_t,
    ffn_taps_hbm,
    down_w,
    result,
    resid,
    gate_in,
    value_in,
    mix_gain,
    conv_taps,
    recur_w,
    input_w,
    decay_rate,
    mlp_gain,
    ffn_taps,
    in_g,
    out_g,
    up_g,
    down_g,
    rows_g,
    gate_w,
    proj,
    gates,
    conv_tail,
    carry,
    recurred,
    pre,
    gate_tail,
    hidden,
    partial,
    from_core,
    to_ring,
    far_in,
    near_in,
    middle,
    w_send,
    w_recv,
    l_sem,
    g_send,
    g_recv,
    c_send,
    c_recv,
    r_send,
    r_recv,
):
    z, x, y, c = (lax.axis_index(a) for a in ("z", "x", "y", "c"))
    at = {"z": z, "x": x, "y": y}

    def nxt(axis, by):
        return lax.rem(at[axis] + (by + RING), RING)

    other = 1 - c
    y_right, y_left, y_far = nxt("y", 1), nxt("y", -1), nxt("y", 2)

    weights = ((in_w, in_g), (out_w, out_g), (None, up_g), (down_w, down_g))

    def own_copy(i):
        if i < 4:
            src, g = weights[i]
            return pltpu.make_async_copy(src, g.at[z, x], l_sem.at[i])
        src, dst = (
            (resid_hbm, resid),
            (gate_t, gate_in),
            (value_t, value_in),
            (mix_gain_hbm, mix_gain),
            (recur_w_hbm, recur_w),
            (input_w_hbm, input_w),
            (conv_taps_hbm, conv_taps),
            (decay_rate_hbm, decay_rate),
            (mlp_gain_hbm, mlp_gain),
            (ffn_taps_hbm, ffn_taps),
        )[i - 4]
        return pltpu.make_async_copy(src, dst, l_sem.at[i])

    for i in (4, 7, 5, 6, 8, 9, 10, 11, 12, 13, 0, 1, 3):
        own_copy(i).start()

    barrier = pltpu.get_barrier_semaphore()
    for axis in ("z", "x", "y"):
        for by in (1, -1):
            pl.semaphore_signal(
                barrier, inc=1, device_id={axis: nxt(axis, by)}, device_id_type=MESH
            )
    pl.semaphore_signal(barrier, inc=1, device_id={"c": other}, device_id_type=MESH)

    def piece(i, p):
        rows = weights[i][1].shape[2] // PIECES[i]
        return pl.ds(p * rows, rows)

    def axes_of(i, p):
        return ("x", "z") if p < X_FIRST[i] else ("z", "x")

    def slot(i, p, axis, by):
        g = weights[i][1]
        if axis == "x":
            return g.at[z, nxt("x", by), piece(i, p)]
        return g.at[nxt("z", by), x, piece(i, p)]

    def line(i, p, axis, by):
        g = weights[i][1]
        if axis == "z":
            return g.at[nxt("z", by), :, piece(i, p)]
        return g.at[:, nxt("x", by), piece(i, p)]

    def w_copy(i, p, src, dst, k, axis, by):
        return remote(
            src, dst, w_send.at[i, k // 3], w_recv.at[i, p, k], **{axis: nxt(axis, by)}
        )

    def first_send(i, p):
        src = weights[i][0]
        axis = axes_of(i, p)[0]
        here = slot(i, p, axis, 0)
        for k, by in ((0, 1), (1, -1)):
            w_copy(i, p, here if src is None else src.at[piece(i, p)], here, k, axis, by).start()

    def first_wait(i, p, k):
        axis = axes_of(i, p)[0]
        there = slot(i, p, axis, (-1, 1, 2)[k])
        w_copy(i, p, there, there, k, axis, 1).wait_recv()

    def first_forward(i, p):
        axis = axes_of(i, p)[0]
        k = p % 2
        first_wait(i, p, k)
        by = 1 if k == 0 else -1
        there = slot(i, p, axis, -by)
        w_copy(i, p, there, there, 2, axis, by).start()

    def second_send(i, p):
        if p == WAITED.get(i):
            own_copy(i).wait()
        axis = axes_of(i, p)[1]
        first_wait(i, p, 1 - p % 2)
        first_wait(i, p, 2)
        here = line(i, p, axis, 0)
        for k, by in ((3, 1), (4, -1)):
            w_copy(i, p, here, here, k, axis, by).start()

    def second_wait(i, p, k):
        axis = axes_of(i, p)[1]
        there = line(i, p, axis, (-1, 1, 2)[k - 3])
        w_copy(i, p, there, there, k, axis, 1).wait_recv()

    def second_forward(i, p):
        axis = axes_of(i, p)[1]
        k = 3 + p % 2
        second_wait(i, p, k)
        by = 1 if k == 3 else -1
        there = line(i, p, axis, -by)
        w_copy(i, p, there, there, 5, axis, by).start()

    def weights_near(i):
        for p in range(PIECES[i]):
            second_wait(i, p, 4 - p % 2)

    def weights_far(i):
        for p in range(PIECES[i]):
            second_wait(i, p, 5)

    def all_sent(ref, sem):
        pltpu.make_async_copy(ref, ref, sem).wait()

    def weights_sent(i):
        g = weights[i][1]
        all_sent(g.at[0, pl.ds(0, 3)], w_send.at[i, 0])
        all_sent(g.at[pl.ds(0, 3)], w_send.at[i, 1])

    def g_copy(n, yq, cq, q, s, r, **device):
        ref = rows_g.at[n, yq, cq, q]
        return remote(ref, ref, g_send.at[n, s // 12], g_recv.at[n, r], **device)

    def rows_wait(n, yq, cq, q, r):
        g_copy(n, yq, cq, q, 0, r, c=other).wait_recv()

    def rows_send(n):
        for q in (0, 1):
            g_copy(n, y, c, q, q, IN_LEFT + q, y=y_right).start()
            g_copy(n, y, c, 1 - q, 2 + 1 - q, IN_RIGHT + 1 - q, y=y_left).start()
            g_copy(n, y, c, q, 4 + q, OWN + q, c=other).start()

    def rows_first(n):
        rows_wait(n, y_left, c, 0, IN_LEFT)
        g_copy(n, y_left, c, 0, 6, IN_FAR, y=y_right).start()
        g_copy(n, y_left, c, 0, 8, LEFT, c=other).start()
        rows_wait(n, y_right, c, 1, IN_RIGHT + 1)
        g_copy(n, y_right, c, 1, 7, IN_FAR + 1, y=y_left).start()
        g_copy(n, y_right, c, 1, 11, RIGHT + 1, c=other).start()

    def rows_second(n):
        rows_wait(n, y_left, c, 1, IN_LEFT + 1)
        g_copy(n, y_left, c, 1, 9, LEFT + 1, c=other).start()
        rows_wait(n, y_right, c, 0, IN_RIGHT)
        g_copy(n, y_right, c, 0, 10, RIGHT, c=other).start()

    def rows_third(n):
        for q in (0, 1):
            rows_wait(n, y_far, c, q, IN_FAR + q)
            g_copy(n, y_far, c, q, 12 + q, FAR + q, c=other).start()

    def rows_sent(n):
        all_sent(rows_g.at[n, pl.ds(0, 3)], g_send.at[n, 0])
        all_sent(rows_g.at[n, 3, 0], g_send.at[n, 1])

    def group(g):
        return (y, y_right) if g == 0 else (y_left, y_far)

    def group_rows(n, g):
        for j, yq in enumerate(group(g)):
            for q in (0, 1):
                rows_wait(n, yq, other, q, 4 * g + 2 * j + q)
        return jnp.concatenate([rows_g[n, yq].reshape(2 * HALF, -1) for yq in group(g)], axis=0)

    def place(t):
        n, lo, hi = SUMS[t]
        return n, pl.ds(lo * 128, (hi - lo) * 128)

    def core_copy(t, yq, k):
        n, cols = place(t)
        return remote(
            partial.at[n, yq, other, :, cols],
            from_core.at[n, yq, :, cols],
            c_send.at[t],
            c_recv.at[t, k],
            c=other,
        )

    def ring_copy(t, j, q, k, side, **device):
        n, cols = place(t)
        there = far_in.at[n, q, :, cols] if side is None else near_in.at[n, side, q, :, cols]
        return remote(to_ring.at[n, j, q, :, cols], there, r_send.at[t], r_recv.at[t, k], **device)

    def chip_sum(t, yq, at_row):
        n, cols = place(t)
        rows = pl.ds(at_row, 16)
        return partial[n, yq, c, rows, cols].astype(F32) + from_core[n, yq, rows, cols].astype(F32)

    def fill_ring(t, j, q, yq, far=False):
        n, cols = place(t)
        for at_row in range(0, QUARTER, 16):
            total = chip_sum(t, yq, q * QUARTER + at_row)
            if far:
                total = total + far_in[n, q, at_row : at_row + 16, cols].astype(F32)
            to_ring[n, j, q, at_row : at_row + 16, cols] = total.astype(BF16)

    def sums_far(t):
        core_copy(t, y_far, 0).wait_recv()
        fill_ring(t, 0, 0, y_far)
        ring_copy(t, 0, 0, 0, None, y=y_right).start()
        fill_ring(t, 0, 1, y_far)
        ring_copy(t, 0, 1, 1, None, y=y_left).start()

    def sums_left(t):
        core_copy(t, y_left, 1).wait_recv()
        fill_ring(t, 1, 0, y_left)
        ring_copy(t, 1, 0, 2, 1, y=y_left).start()

    def sums_right(t):
        core_copy(t, y_right, 2).wait_recv()
        fill_ring(t, 2, 1, y_right)
        ring_copy(t, 2, 1, 3, 0, y=y_right).start()

    def sums_near(t):
        ring_copy(t, 0, 0, 0, None, y=y_right).wait_recv()
        fill_ring(t, 2, 0, y_right, True)
        ring_copy(t, 2, 0, 4, 0, y=y_right).start()
        ring_copy(t, 0, 1, 1, None, y=y_left).wait_recv()
        fill_ring(t, 1, 1, y_left, True)
        ring_copy(t, 1, 1, 5, 1, y=y_left).start()

    def sums_sent(t):
        n, cols = place(t)
        all_sent(from_core.at[n, :, :, cols], c_send.at[t])
        all_sent(to_ring.at[n, :, :, :, cols], r_send.at[t])

    def sums_wait(t):
        core_copy(t, y, 3).wait_recv()
        for side in (0, 1):
            for q in (0, 1):
                k = ((4, 3), (2, 5))[side][q]
                ring_copy(t, 0, q, k, side, y=y_right).wait_recv()

    def own_sum(t, q, at_row):
        n, cols = place(t)
        total = chip_sum(t, y, q * QUARTER + at_row)
        for side in (0, 1):
            total = total + near_in[n, side, q, at_row : at_row + 16, cols].astype(F32)
        return total

    def first_norm(h):
        for q in (0, 1):
            for at_row in range(0, QUARTER, 16):
                here = h * HALF + q * QUARTER + at_row
                wide = resid[here : here + 16, :].astype(F32)
                rows_g[h, y, c, q, at_row : at_row + 16, :] = rms_rows(wide, mix_gain[...])

    def gate_map():
        gate_w[...] = jnp.zeros_like(gate_w)
        for n in range(recur_w.shape[0]):
            block = slice(n * GATE_BLOCK, (n + 1) * GATE_BLOCK)
            gate_w[block, block] = recur_w[n]
            block_two = slice(256 + n * GATE_BLOCK, 256 + (n + 1) * GATE_BLOCK)
            gate_w[block, block_two] = input_w[n]

    def turn_up():
        for b in range(11):
            if b < 5:
                tile = gate_in[b * 128 : (b + 1) * 128, :]
            elif b < 10:
                tile = value_in[(b - 5) * 128 : (b - 4) * 128, :]
            else:
                tile = jnp.concatenate([gate_in[640:704, :], value_in[640:704, :]], axis=0)
            up_g[z, x, :, b * 128 : (b + 1) * 128] = tile.astype(F32).T.astype(BF16)

    def recur(h, g):
        w = in_g[...].reshape(-1, 256)
        proj[...] = jnp.dot(group_rows(h, g), w, preferred_element_type=F32)
        taps = conv_taps[...]
        blocks = [(j, s) for j in range(2) for s in range(2)]
        for j, s in blocks:
            yq = group(g)[j]
            rows = slice((2 * j + s) * HALF, (2 * j + s + 1) * HALF)
            wide = proj[rows, :].astype(BF16).astype(F32)
            before = jnp.zeros((8, 256), F32) if h == 0 else conv_tail[yq, s]
            if h == 0:
                conv_tail[yq, s] = wide[HALF - 8 :]
            extended = jnp.concatenate([before, wide], axis=0)
            conv = behind(extended, 3) * taps[0:1]
            conv = conv + behind(extended, 2) * taps[1:2]
            conv = conv + behind(extended, 1) * taps[2:3]
            proj[rows, :] = conv + wide * taps[3:4]
        gates[...] = jnp.dot(proj[...].astype(BF16), gate_w[...], preferred_element_type=F32)
        for j, s in blocks:
            yq = group(g)[j]
            rows = slice((2 * j + s) * HALF, (2 * j + s + 1) * HALF)
            for b in range(2):
                lanes = slice(b * 128, (b + 1) * 128)
                lanes2 = slice(256 + b * 128, 256 + (b + 1) * 128)
                rgate = jax.nn.sigmoid(gates[rows, lanes])
                igate = jax.nn.sigmoid(gates[rows, lanes2])
                a = 8.0 * rgate * decay_rate[:, lanes]
                decay = jnp.exp(-a)
                a2 = a * a
                series = 1.0 + a2 * (1.0 / 6) * (1.0 + a2 * (1.0 / 20) * (1.0 + a2 * (1.0 / 42)))
                left_over = jnp.where(a < 0.3, 2.0 * decay * (a * series), 1.0 - decay * decay)
                state = jnp.sqrt(left_over) * (igate * proj[rows, lanes])
                pos = lax.broadcasted_iota(jnp.int32, state.shape, 0)
                if h == 1:
                    state = state + jnp.where(pos == 0, decay * carry[yq, s, 0:1, lanes], 0.0)
                by = 1
                while by < HALF:
                    state = decay * shifted(state, pos, by, 0.0) + state
                    if 2 * by < HALF:
                        decay = decay * shifted(decay, pos, by, 1.0)
                    by *= 2
                if h == 0:
                    carry[yq, s, 0:1, lanes] = state[HALF - 1 :]
                recurred[h, yq, s * HALF : (s + 1) * HALF, lanes] = state.astype(BF16)

    def step_product(t, g):
        n, lo, hi = SUMS[t]
        left, table = (recurred, out_g) if n < 2 else (hidden, down_g)
        rows = jnp.concatenate([left[n % 2, yq] for yq in group(g)], axis=0)
        for b in range(lo, hi, 4):
            end = min(b + 4, hi)
            w = []
            for d in range(b, end):
                if n < 2:
                    w.append(table[d // RING, d % RING])
                else:
                    w.append(table[nxt("z", BLOCKS[d][0]), nxt("x", BLOCKS[d][1])])
            term = jnp.dot(rows, jnp.concatenate(w, axis=1), preferred_element_type=F32)
            term = term.astype(BF16)
            for j, yq in enumerate(group(g)):
                for s in range(2):
                    at_row = (2 * j + s) * HALF
                    partial[n, yq, s, :, b * 128 : end * 128] = term[at_row : at_row + HALF]
        for j, k in ((1, 2), (0, 3)) if g == 0 else ((1, 0), (0, 1)):
            core_copy(t, group(g)[j], k).start()

    def second_norm(h):
        sums_wait(h)
        for q in (0, 1):
            for at_row in range(0, QUARTER, 16):
                lo = h * HALF + q * QUARTER + at_row
                here = slice(lo, lo + 16)
                mid = (resid[here, :].astype(F32) + own_sum(h, q, at_row)).astype(BF16)
                middle[here, :] = mid
                out = rms_rows(mid.astype(F32), mlp_gain[...])
                rows_g[2 + h, y, c, q, at_row : at_row + 16, :] = out

    def gated(extended, value, taps):
        conv = behind(extended, 2) * taps[0:1]
        conv = conv + behind(extended, 1) * taps[1:2]
        conv = conv + extended[8:] * taps[2:3]
        return (conv / (1.0 + jnp.exp(-conv)) * value).astype(BF16)

    def feed(h, g):
        w = up_g[...].reshape(-1, 1408)
        pre[...] = jnp.dot(group_rows(2 + h, g), w, preferred_element_type=F32)
        for j in range(2):
            yq = group(g)[j]
            for s in range(2):
                rows = slice((2 * j + s) * HALF, (2 * j + s + 1) * HALF)
                out = slice(s * HALF, (s + 1) * HALF)
                for b in range(6):
                    lanes = slice(b * 128, (b + 1) * 128)
                    if b < 5:
                        gate = pre[rows, lanes].astype(BF16).astype(F32)
                        value = pre[rows, 640 + b * 128 : 640 + (b + 1) * 128]
                        value = value.astype(BF16).astype(F32)
                        taps = ffn_taps[:, lanes]
                    else:
                        gate = pre[rows, 1280:1408].astype(BF16).astype(F32)
                        value = pltpu.roll(gate, 64, axis=1)
                        taps = jnp.concatenate([ffn_taps[:, 640:704], jnp.zeros((3, 64), F32)], axis=1)
                    before = jnp.zeros((8, 128), F32) if h == 0 else gate_tail[yq, s, :, lanes]
                    if h == 0:
                        gate_tail[yq, s, :, lanes] = gate[HALF - 8 :]
                    unit = gated(jnp.concatenate([before, gate], axis=0), value, taps)
                    if b < 5:
                        hidden[h, yq, out, lanes] = unit
                    else:
                        hidden[h, yq, out, 640:704] = unit[:, :64]

    def finish(t):
        n, lo, hi = SUMS[t]
        sums_wait(t)
        for q in (0, 1):
            for at_row in range(0, QUARTER, 16):
                here = pl.ds((n - 2) * HALF + q * QUARTER + at_row, 16)
                total = own_sum(t, q, at_row)
                for b in range(lo, hi):
                    at_col = nxt("z", BLOCKS[b][0]) * 512 + nxt("x", BLOCKS[b][1]) * 128
                    cols = pl.ds(pl.multiple_of(at_col, 128), 128)
                    part = total[:, (b - lo) * 128 : (b - lo + 1) * 128]
                    result[here, cols] = (middle[here, cols].astype(F32) + part).astype(BF16)

    own_copy(4).wait()
    own_copy(7).wait()
    first_norm(0)
    own_copy(5).wait()
    own_copy(6).wait()
    turn_up()
    own_copy(8).wait()
    own_copy(9).wait()
    gate_map()
    first_norm(1)
    for i in (10, 11, 12, 13):
        own_copy(i).wait()
    pl.semaphore_wait(barrier, 7)

    def sent():
        for n in range(4):
            rows_sent(n)
        for t in range(5):
            sums_sent(t)
        for i in range(4):
            weights_sent(i)

    steps = {
        "S1": first_send,
        "F1": first_forward,
        "S2": second_send,
        "F2": second_forward,
        "DA": weights_near,
        "DB": weights_far,
        "RS": rows_send,
        "R1": rows_first,
        "R2": rows_second,
        "R3": rows_third,
        "rec": recur,
        "feed": feed,
        "prod": step_product,
        "sfar": sums_far,
        "sleft": sums_left,
        "sright": sums_right,
        "near": sums_near,
        "norm2": second_norm,
        "fin": finish,
        "sent": sent,
    }
    for name, *where in ORDER:
        steps[name](*where)
    sums_sent(5)


def shards(
    resid,
    mix_gain,
    in_weight,
    conv_taps,
    recur_gate_w,
    input_gate_w,
    decay_rate,
    out_weight,
    mlp_gain,
    up_gate_w,
    up_val_w,
    ffn_taps,
    down_weight,
):
    hbm = pl.BlockSpec(memory_space=pl.ANY)
    dma = pltpu.SemaphoreType.DMA
    width = resid.shape[1]
    units = up_gate_w.shape[1]
    return pl.pallas_call(
        kernel,
        name="layer",
        out_shape=pltpu.VMEM(resid.shape, BF16),
        in_specs=[hbm] * 13,
        out_specs=pl.BlockSpec(memory_space=pltpu.VMEM),
        scratch_shapes=[
            pltpu.VMEM(resid.shape, BF16),
            pltpu.VMEM((units, 128), BF16),
            pltpu.VMEM((units, 128), BF16),
            pltpu.VMEM((1, width), F32),
            pltpu.VMEM(conv_taps.shape, F32),
            pltpu.VMEM(recur_gate_w.shape, BF16),
            pltpu.VMEM(input_gate_w.shape, BF16),
            pltpu.VMEM((1, *decay_rate.shape), F32),
            pltpu.VMEM((1, width), F32),
            pltpu.VMEM(ffn_taps.shape, F32),
            pltpu.VMEM((RING, RING, *in_weight.shape), BF16),
            pltpu.VMEM((RING, RING, *out_weight.shape), BF16),
            pltpu.VMEM((RING, RING, up_gate_w.shape[0], 2 * units), BF16),
            pltpu.VMEM((RING, RING, *down_weight.shape), BF16),
            pltpu.VMEM((4, RING, 2, 2, QUARTER, width), BF16),
            pltpu.VMEM((256, 512), BF16),
            pltpu.VMEM((4 * HALF, 256), F32),
            pltpu.VMEM((4 * HALF, 512), F32),
            pltpu.VMEM((RING, 2, 8, 256), F32),
            pltpu.VMEM((RING, 2, 8, 256), F32),
            pltpu.VMEM((2, RING, 2 * HALF, 256), BF16),
            pltpu.VMEM((4 * HALF, 2 * units), F32),
            pltpu.VMEM((RING, 2, 8, 768), F32),
            pltpu.VMEM((2, RING, 2 * HALF, units), BF16),
            pltpu.VMEM((4, RING, 2, HALF, width), BF16),
            pltpu.VMEM((4, RING, HALF, width), BF16),
            pltpu.VMEM((4, 3, 2, QUARTER, width), BF16),
            pltpu.VMEM((4, 2, QUARTER, width), BF16),
            pltpu.VMEM((4, 2, 2, QUARTER, width), BF16),
            pltpu.VMEM((SEQ, width), BF16),
            dma((4, 2)),
            dma((4, max(PIECES), 6)),
            dma((14,)),
            dma((4, 2)),
            dma((4, 14)),
            dma((6,)),
            dma((6, 4)),
            dma((6,)),
            dma((6, 6)),
        ],
        compiler_params=pltpu.CompilerParams(
            collective_id=0, has_side_effects=True, vmem_limit_bytes=56 * 1024 * 1024
        ),
    )(
        resid,
        mix_gain[None],
        in_weight,
        conv_taps,
        recur_gate_w,
        input_gate_w,
        decay_rate[None],
        out_weight,
        mlp_gain[None],
        up_gate_w.T,
        up_val_w.T,
        ffn_taps,
        down_weight,
    )


def solution(mesh):
    split = Mesh(mesh.devices.reshape(RING, RING, RING, 2), ("z", "x", "y", "c"))
    fs, tp = ("z", "x"), ("y", "c")
    rows = ("z", "x", "y", "c")
    return jax.shard_map(
        shards,
        mesh=split,
        in_specs=(
            P(rows, None),
            P(),
            P(fs, tp),
            P(None, tp),
            P(tp, None, None),
            P(tp, None, None),
            P(tp),
            P(tp, fs),
            P(),
            P(fs, tp),
            P(fs, tp),
            P(None, tp),
            P(tp, fs),
        ),
        out_specs=P(rows, None),
        check_vma=False,
    )
```

```python
import jax
import jax.numpy as jnp
from jax import lax
from jax.experimental import pallas as pl
from jax.experimental.pallas import tpu as pltpu
from jax.sharding import Mesh
from jax.sharding import PartitionSpec as P

GATE_BLOCK = 64
SEQ = 128
HALF = 64
QUARTER = 32
RING = 4
MESH = pl.DeviceIdType.MESH
BF16 = jnp.bfloat16
F32 = jnp.float32

OWN, RIGHT, LEFT, FAR, IN_RIGHT, IN_LEFT, IN_FAR = 0, 2, 4, 6, 8, 10, 12


PIECES = (4, 4, 4, 4)
X_FIRST = (2, 2, 2, 2)
DIRECT = (True, True, False, False)
SUMS = ((0, 0, 16), (1, 0, 16), (2, 0, 9), (3, 0, 9), (2, 9, 16), (3, 9, 16))
BLOCKS = tuple(
    sorted(((dz, dx) for dz in (0, 1, -1, 2) for dx in (0, 1, -1, 2)), key=lambda d: 2 in d)
)
ORDER = (
    ("S1", 3, 3),
    ("S1", 2, 1),
    ("S1", 1, 2),
    ("S1", 0, 0),
    ("RS", 0),
    ("S1", 0, 2),
    ("S1", 0, 3),
    ("S1", 1, 0),
    ("S1", 0, 1),
    ("S1", 1, 1),
    ("S1", 1, 3),
    ("S1", 2, 2),
    ("F1", 0, 0),
    ("S1", 2, 0),
    ("F1", 0, 2),
    ("RS", 1),
    ("S1", 2, 3),
    ("F1", 0, 3),
    ("F1", 1, 3),
    ("F1", 0, 1),
    ("S2", 0, 0),
    ("F1", 1, 0),
    ("S2", 0, 2),
    ("S2", 0, 3),
    ("S2", 1, 3),
    ("S2", 1, 0),
    ("F1", 1, 2),
    ("S2", 1, 2),
    ("F1", 1, 1),
    ("S2", 0, 1),
    ("F1", 2, 0),
    ("F2", 0, 0),
    ("S2", 1, 1),
    ("F2", 0, 2),
    ("R1", 0),
    ("R2", 0),
    ("S1", 3, 1),
    ("F2", 0, 3),
    ("F1", 2, 3),
    ("F1", 2, 1),
    ("F1", 2, 2),
    ("F2", 0, 1),
    ("F2", 1, 1),
    ("R1", 1),
    ("F2", 1, 2),
    ("F2", 1, 0),
    ("F2", 1, 3),
    ("R2", 1),
    ("S1", 3, 0),
    ("R3", 0),
    ("S1", 3, 2),
    ("S2", 2, 0),
    ("DA", 0),
    ("DA", 1),
    ("F1", 3, 1),
    ("S2", 2, 3),
    ("DB", 0),
    ("rec", 0, 1),
    ("DB", 1),
    ("prod", 0, 1),
    ("rec", 0, 0),
    ("sfar", 0),
    ("R3", 1),
    ("F1", 3, 2),
    ("S2", 2, 1),
    ("prod", 0, 0),
    ("sleft", 0),
    ("sright", 0),
    ("S2", 2, 2),
    ("rec", 1, 1),
    ("prod", 1, 1),
    ("near", 0),
    ("rec", 1, 0),
    ("sfar", 1),
    ("prod", 1, 0),
    ("sleft", 1),
    ("F2", 2, 0),
    ("F2", 2, 3),
    ("S2", 3, 1),
    ("sright", 1),
    ("S2", 3, 2),
    ("F1", 3, 0),
    ("near", 1),
    ("F1", 3, 3),
    ("norm2", 0),
    ("RS", 2),
    ("F2", 2, 1),
    ("F2", 2, 2),
    ("R1", 2),
    ("S2", 3, 3),
    ("S2", 3, 0),
    ("norm2", 1),
    ("RS", 3),
    ("F2", 3, 2),
    ("R2", 2),
    ("R3", 2),
    ("DA", 2),
    ("DB", 2),
    ("F2", 3, 1),
    ("feed", 0, 0),
    ("F2", 3, 0),
    ("F2", 3, 3),
    ("R1", 3),
    ("DA", 3),
    ("feed", 0, 1),
    ("prod", 2, 0),
    ("prod", 2, 1),
    ("R2", 3),
    ("sfar", 2),
    ("R3", 3),
    ("DB", 3),
    ("prod", 4, 1),
    ("prod", 4, 0),
    ("sright", 2),
    ("sleft", 2),
    ("sfar", 4),
    ("feed", 1, 1),
    ("sright", 4),
    ("sleft", 4),
    ("prod", 3, 1),
    ("near", 2),
    ("prod", 5, 1),
    ("near", 4),
    ("sfar", 3),
    ("feed", 1, 0),
    ("prod", 3, 0),
    ("sfar", 5),
    ("sleft", 5),
    ("sright", 3),
    ("sleft", 3),
    ("fin", 2),
    ("prod", 5, 0),
    ("near", 3),
    ("sent",),
    ("fin", 4),
    ("sright", 5),
    ("near", 5),
    ("fin", 3),
    ("fin", 5),
)
WAITED = {0: 0, 1: 3, 3: 1}


def remote(src, dst, send_sem, recv_sem, **device):
    return pltpu.make_async_remote_copy(
        src_ref=src,
        dst_ref=dst,
        send_sem=send_sem,
        recv_sem=recv_sem,
        device_id=device,
        device_id_type=MESH,
    )


def rms_rows(wide, gain):
    scale = lax.rsqrt(jnp.mean(wide * wide, axis=-1, keepdims=True) + 1e-06)
    return (wide * scale * gain).astype(BF16)


def shifted(values, rows, by, fill):
    return jnp.where(rows >= by, pltpu.roll(values, by, axis=0), fill)


def behind(extended, by):
    return pltpu.roll(extended, by, axis=0)[8:]


def kernel(
    resid_hbm,
    mix_gain_hbm,
    in_w,
    conv_taps_hbm,
    recur_w_hbm,
    input_w_hbm,
    decay_rate_hbm,
    out_w,
    mlp_gain_hbm,
    gate_t,
    value_t,
    ffn_taps_hbm,
    down_w,
    result,
    resid,
    gate_in,
    value_in,
    mix_gain,
    conv_taps,
    recur_w,
    input_w,
    decay_rate,
    mlp_gain,
    ffn_taps,
    in_g,
    out_g,
    up_g,
    down_g,
    rows_g,
    gate_w,
    proj,
    gates,
    conv_tail,
    carry,
    recurred,
    pre,
    gate_tail,
    hidden,
    partial,
    from_core,
    to_ring,
    far_in,
    near_in,
    middle,
    w_send,
    w_recv,
    l_sem,
    g_send,
    g_recv,
    c_send,
    c_recv,
    r_send,
    r_recv,
):
    z, x, y, c = (lax.axis_index(a) for a in ("z", "x", "y", "c"))
    at = {"z": z, "x": x, "y": y}

    def nxt(axis, by):
        return lax.rem(at[axis] + (by + RING), RING)

    other = 1 - c
    y_right, y_left, y_far = nxt("y", 1), nxt("y", -1), nxt("y", 2)

    weights = ((in_w, in_g), (out_w, out_g), (None, up_g), (down_w, down_g))

    def own_copy(i):
        if i < 4:
            src, g = weights[i]
            return pltpu.make_async_copy(src, g.at[z, x], l_sem.at[i])
        src, dst = (
            (resid_hbm, resid),
            (gate_t, gate_in),
            (value_t, value_in),
            (mix_gain_hbm, mix_gain),
            (recur_w_hbm, recur_w),
            (input_w_hbm, input_w),
            (conv_taps_hbm, conv_taps),
            (decay_rate_hbm, decay_rate),
            (mlp_gain_hbm, mlp_gain),
            (ffn_taps_hbm, ffn_taps),
        )[i - 4]
        return pltpu.make_async_copy(src, dst, l_sem.at[i])

    for i in (4, 7, 5, 6, 8, 9, 10, 11, 12, 13, 0, 1, 3):
        own_copy(i).start()

    barrier = pltpu.get_barrier_semaphore()
    for axis in ("z", "x", "y"):
        for by in (1, -1) if axis == "y" else (1, -1, 2):
            pl.semaphore_signal(
                barrier, inc=1, device_id={axis: nxt(axis, by)}, device_id_type=MESH
            )
    pl.semaphore_signal(barrier, inc=1, device_id={"c": other}, device_id_type=MESH)

    def piece(i, p):
        rows = weights[i][1].shape[2] // PIECES[i]
        return pl.ds(p * rows, rows)

    def axes_of(i, p):
        return ("x", "z") if p < X_FIRST[i] else ("z", "x")

    def slot(i, p, axis, by):
        g = weights[i][1]
        if axis == "x":
            return g.at[z, nxt("x", by), piece(i, p)]
        return g.at[nxt("z", by), x, piece(i, p)]

    def line(i, p, axis, by):
        g = weights[i][1]
        if axis == "z":
            return g.at[nxt("z", by), :, piece(i, p)]
        return g.at[:, nxt("x", by), piece(i, p)]

    def w_copy(i, p, src, dst, k, axis, by):
        return remote(
            src, dst, w_send.at[i, k // 3], w_recv.at[i, p, k], **{axis: nxt(axis, by)}
        )

    def first_send(i, p):
        src = weights[i][0]
        axis = axes_of(i, p)[0]
        here = slot(i, p, axis, 0)
        for k, by in ((0, 1), (1, -1), (2, 2))[: 3 if DIRECT[i] else 2]:
            w_copy(i, p, here if src is None else src.at[piece(i, p)], here, k, axis, by).start()

    def first_wait(i, p, k):
        axis = axes_of(i, p)[0]
        there = slot(i, p, axis, (-1, 1, 2)[k])
        w_copy(i, p, there, there, k, axis, 1).wait_recv()

    def first_forward(i, p):
        axis = axes_of(i, p)[0]
        k = p % 2
        first_wait(i, p, k)
        by = 1 if k == 0 else -1
        there = slot(i, p, axis, -by)
        if not DIRECT[i]:
            w_copy(i, p, there, there, 2, axis, by).start()

    def second_send(i, p):
        if p == WAITED.get(i):
            own_copy(i).wait()
        axis = axes_of(i, p)[1]
        first_wait(i, p, 1 - p % 2)
        first_wait(i, p, 2)
        here = line(i, p, axis, 0)
        for k, by in ((3, 1), (4, -1)):
            w_copy(i, p, here, here, k, axis, by).start()

    def second_wait(i, p, k):
        axis = axes_of(i, p)[1]
        there = line(i, p, axis, (-1, 1, 2)[k - 3])
        w_copy(i, p, there, there, k, axis, 1).wait_recv()

    def second_forward(i, p):
        axis = axes_of(i, p)[1]
        k = 3 + p % 2
        second_wait(i, p, k)
        by = 1 if k == 3 else -1
        there = line(i, p, axis, -by)
        w_copy(i, p, there, there, 5, axis, by).start()

    def weights_near(i):
        for p in range(PIECES[i]):
            second_wait(i, p, 4 - p % 2)

    def weights_far(i):
        for p in range(PIECES[i]):
            second_wait(i, p, 5)

    def all_sent(ref, sem):
        pltpu.make_async_copy(ref, ref, sem).wait()

    def weights_sent(i):
        g = weights[i][1]
        all_sent(g.at[0, pl.ds(0, 3)], w_send.at[i, 0])
        all_sent(g.at[pl.ds(0, 3)], w_send.at[i, 1])

    def g_copy(n, yq, cq, q, s, r, **device):
        ref = rows_g.at[n, yq, cq, q]
        return remote(ref, ref, g_send.at[n, s // 12], g_recv.at[n, r], **device)

    def rows_wait(n, yq, cq, q, r):
        g_copy(n, yq, cq, q, 0, r, c=other).wait_recv()

    def rows_send(n):
        for q in (0, 1):
            g_copy(n, y, c, q, q, IN_LEFT + q, y=y_right).start()
            g_copy(n, y, c, 1 - q, 2 + 1 - q, IN_RIGHT + 1 - q, y=y_left).start()
            g_copy(n, y, c, q, 4 + q, OWN + q, c=other).start()

    def rows_first(n):
        rows_wait(n, y_left, c, 0, IN_LEFT)
        g_copy(n, y_left, c, 0, 6, IN_FAR, y=y_right).start()
        g_copy(n, y_left, c, 0, 8, LEFT, c=other).start()
        rows_wait(n, y_right, c, 1, IN_RIGHT + 1)
        g_copy(n, y_right, c, 1, 7, IN_FAR + 1, y=y_left).start()
        g_copy(n, y_right, c, 1, 11, RIGHT + 1, c=other).start()

    def rows_second(n):
        rows_wait(n, y_left, c, 1, IN_LEFT + 1)
        g_copy(n, y_left, c, 1, 9, LEFT + 1, c=other).start()
        rows_wait(n, y_right, c, 0, IN_RIGHT)
        g_copy(n, y_right, c, 0, 10, RIGHT, c=other).start()

    def rows_third(n):
        for q in (0, 1):
            rows_wait(n, y_far, c, q, IN_FAR + q)
            g_copy(n, y_far, c, q, 12 + q, FAR + q, c=other).start()

    def rows_sent(n):
        all_sent(rows_g.at[n, pl.ds(0, 3)], g_send.at[n, 0])
        all_sent(rows_g.at[n, 3, 0], g_send.at[n, 1])

    def group(g):
        return (y, y_right) if g == 0 else (y_left, y_far)

    def group_rows(n, g):
        for j, yq in enumerate(group(g)):
            for q in (0, 1):
                rows_wait(n, yq, other, q, 4 * g + 2 * j + q)
        return jnp.concatenate([rows_g[n, yq].reshape(2 * HALF, -1) for yq in group(g)], axis=0)

    def place(t):
        n, lo, hi = SUMS[t]
        return n, pl.ds(lo * 128, (hi - lo) * 128)

    def core_copy(t, yq, k):
        n, cols = place(t)
        return remote(
            partial.at[n, yq, other, :, cols],
            from_core.at[n, yq, :, cols],
            c_send.at[t],
            c_recv.at[t, k],
            c=other,
        )

    def ring_copy(t, j, q, k, side, **device):
        n, cols = place(t)
        there = far_in.at[n, q, :, cols] if side is None else near_in.at[n, side, q, :, cols]
        return remote(to_ring.at[n, j, q, :, cols], there, r_send.at[t], r_recv.at[t, k], **device)

    def chip_sum(t, yq, at_row):
        n, cols = place(t)
        rows = pl.ds(at_row, 16)
        return partial[n, yq, c, rows, cols].astype(F32) + from_core[n, yq, rows, cols].astype(F32)

    def fill_ring(t, j, q, yq, far=False):
        n, cols = place(t)
        for at_row in range(0, QUARTER, 16):
            total = chip_sum(t, yq, q * QUARTER + at_row)
            if far:
                total = total + far_in[n, q, at_row : at_row + 16, cols].astype(F32)
            to_ring[n, j, q, at_row : at_row + 16, cols] = total.astype(BF16)

    def sums_far(t):
        core_copy(t, y_far, 0).wait_recv()
        fill_ring(t, 0, 0, y_far)
        ring_copy(t, 0, 0, 0, None, y=y_right).start()
        fill_ring(t, 0, 1, y_far)
        ring_copy(t, 0, 1, 1, None, y=y_left).start()

    def sums_left(t):
        core_copy(t, y_left, 1).wait_recv()
        fill_ring(t, 1, 0, y_left)
        ring_copy(t, 1, 0, 2, 1, y=y_left).start()

    def sums_right(t):
        core_copy(t, y_right, 2).wait_recv()
        fill_ring(t, 2, 1, y_right)
        ring_copy(t, 2, 1, 3, 0, y=y_right).start()

    def sums_near(t):
        ring_copy(t, 0, 0, 0, None, y=y_right).wait_recv()
        fill_ring(t, 2, 0, y_right, True)
        ring_copy(t, 2, 0, 4, 0, y=y_right).start()
        ring_copy(t, 0, 1, 1, None, y=y_left).wait_recv()
        fill_ring(t, 1, 1, y_left, True)
        ring_copy(t, 1, 1, 5, 1, y=y_left).start()

    def sums_sent(t):
        n, cols = place(t)
        all_sent(from_core.at[n, :, :, cols], c_send.at[t])
        all_sent(to_ring.at[n, :, :, :, cols], r_send.at[t])

    def sums_wait(t):
        core_copy(t, y, 3).wait_recv()
        for side in (0, 1):
            for q in (0, 1):
                k = ((4, 3), (2, 5))[side][q]
                ring_copy(t, 0, q, k, side, y=y_right).wait_recv()

    def own_sum(t, q, at_row):
        n, cols = place(t)
        total = chip_sum(t, y, q * QUARTER + at_row)
        for side in (0, 1):
            total = total + near_in[n, side, q, at_row : at_row + 16, cols].astype(F32)
        return total

    def first_norm(h):
        for q in (0, 1):
            for at_row in range(0, QUARTER, 16):
                here = h * HALF + q * QUARTER + at_row
                wide = resid[here : here + 16, :].astype(F32)
                rows_g[h, y, c, q, at_row : at_row + 16, :] = rms_rows(wide, mix_gain[...])

    def gate_map():
        gate_w[...] = jnp.zeros_like(gate_w)
        for n in range(recur_w.shape[0]):
            block = slice(n * GATE_BLOCK, (n + 1) * GATE_BLOCK)
            gate_w[block, block] = recur_w[n]
            block_two = slice(256 + n * GATE_BLOCK, 256 + (n + 1) * GATE_BLOCK)
            gate_w[block, block_two] = input_w[n]

    def turn_up():
        for b in range(11):
            if b < 5:
                tile = gate_in[b * 128 : (b + 1) * 128, :]
            elif b < 10:
                tile = value_in[(b - 5) * 128 : (b - 4) * 128, :]
            else:
                tile = jnp.concatenate([gate_in[640:704, :], value_in[640:704, :]], axis=0)
            up_g[z, x, :, b * 128 : (b + 1) * 128] = tile.astype(F32).T.astype(BF16)

    def recur(h, g):
        w = in_g[...].reshape(-1, 256)
        proj[...] = jnp.dot(group_rows(h, g), w, preferred_element_type=F32)
        taps = conv_taps[...]
        blocks = [(j, s) for j in range(2) for s in range(2)]
        for j, s in blocks:
            yq = group(g)[j]
            rows = slice((2 * j + s) * HALF, (2 * j + s + 1) * HALF)
            wide = proj[rows, :].astype(BF16).astype(F32)
            before = jnp.zeros((8, 256), F32) if h == 0 else conv_tail[yq, s]
            if h == 0:
                conv_tail[yq, s] = wide[HALF - 8 :]
            extended = jnp.concatenate([before, wide], axis=0)
            conv = behind(extended, 3) * taps[0:1]
            conv = conv + behind(extended, 2) * taps[1:2]
            conv = conv + behind(extended, 1) * taps[2:3]
            proj[rows, :] = conv + wide * taps[3:4]
        gates[...] = jnp.dot(proj[...].astype(BF16), gate_w[...], preferred_element_type=F32)
        for j, s in blocks:
            yq = group(g)[j]
            rows = slice((2 * j + s) * HALF, (2 * j + s + 1) * HALF)
            for b in range(2):
                lanes = slice(b * 128, (b + 1) * 128)
                lanes2 = slice(256 + b * 128, 256 + (b + 1) * 128)
                rgate = jax.nn.sigmoid(gates[rows, lanes])
                igate = jax.nn.sigmoid(gates[rows, lanes2])
                a = 8.0 * rgate * decay_rate[:, lanes]
                decay = jnp.exp(-a)
                a2 = a * a
                series = 1.0 + a2 * (1.0 / 6) * (1.0 + a2 * (1.0 / 20) * (1.0 + a2 * (1.0 / 42)))
                left_over = jnp.where(a < 0.3, 2.0 * decay * (a * series), 1.0 - decay * decay)
                state = jnp.sqrt(left_over) * (igate * proj[rows, lanes])
                pos = lax.broadcasted_iota(jnp.int32, state.shape, 0)
                if h == 1:
                    state = state + jnp.where(pos == 0, decay * carry[yq, s, 0:1, lanes], 0.0)
                by = 1
                while by < HALF:
                    state = decay * shifted(state, pos, by, 0.0) + state
                    if 2 * by < HALF:
                        decay = decay * shifted(decay, pos, by, 1.0)
                    by *= 2
                if h == 0:
                    carry[yq, s, 0:1, lanes] = state[HALF - 1 :]
                recurred[h, yq, s * HALF : (s + 1) * HALF, lanes] = state.astype(BF16)

    def step_product(t, g):
        n, lo, hi = SUMS[t]
        left, table = (recurred, out_g) if n < 2 else (hidden, down_g)
        rows = jnp.concatenate([left[n % 2, yq] for yq in group(g)], axis=0)
        for b in range(lo, hi, 4):
            end = min(b + 4, hi)
            w = []
            for d in range(b, end):
                if n < 2:
                    w.append(table[d // RING, d % RING])
                else:
                    w.append(table[nxt("z", BLOCKS[d][0]), nxt("x", BLOCKS[d][1])])
            term = jnp.dot(rows, jnp.concatenate(w, axis=1), preferred_element_type=F32)
            term = term.astype(BF16)
            for j, yq in enumerate(group(g)):
                for s in range(2):
                    at_row = (2 * j + s) * HALF
                    partial[n, yq, s, :, b * 128 : end * 128] = term[at_row : at_row + HALF]
        for j, k in ((1, 2), (0, 3)) if g == 0 else ((1, 0), (0, 1)):
            core_copy(t, group(g)[j], k).start()

    def second_norm(h):
        sums_wait(h)
        for q in (0, 1):
            for at_row in range(0, QUARTER, 16):
                lo = h * HALF + q * QUARTER + at_row
                here = slice(lo, lo + 16)
                mid = (resid[here, :].astype(F32) + own_sum(h, q, at_row)).astype(BF16)
                middle[here, :] = mid
                out = rms_rows(mid.astype(F32), mlp_gain[...])
                rows_g[2 + h, y, c, q, at_row : at_row + 16, :] = out

    def gated(extended, value, taps):
        conv = behind(extended, 2) * taps[0:1]
        conv = conv + behind(extended, 1) * taps[1:2]
        conv = conv + extended[8:] * taps[2:3]
        return (conv / (1.0 + jnp.exp(-conv)) * value).astype(BF16)

    def feed(h, g):
        w = up_g[...].reshape(-1, 1408)
        pre[...] = jnp.dot(group_rows(2 + h, g), w, preferred_element_type=F32)
        for j in range(2):
            yq = group(g)[j]
            for s in range(2):
                rows = slice((2 * j + s) * HALF, (2 * j + s + 1) * HALF)
                out = slice(s * HALF, (s + 1) * HALF)
                for b in range(6):
                    lanes = slice(b * 128, (b + 1) * 128)
                    if b < 5:
                        gate = pre[rows, lanes].astype(BF16).astype(F32)
                        value = pre[rows, 640 + b * 128 : 640 + (b + 1) * 128]
                        value = value.astype(BF16).astype(F32)
                        taps = ffn_taps[:, lanes]
                    else:
                        gate = pre[rows, 1280:1408].astype(BF16).astype(F32)
                        value = pltpu.roll(gate, 64, axis=1)
                        taps = jnp.concatenate([ffn_taps[:, 640:704], jnp.zeros((3, 64), F32)], axis=1)
                    before = jnp.zeros((8, 128), F32) if h == 0 else gate_tail[yq, s, :, lanes]
                    if h == 0:
                        gate_tail[yq, s, :, lanes] = gate[HALF - 8 :]
                    unit = gated(jnp.concatenate([before, gate], axis=0), value, taps)
                    if b < 5:
                        hidden[h, yq, out, lanes] = unit
                    else:
                        hidden[h, yq, out, 640:704] = unit[:, :64]

    def finish(t):
        n, lo, hi = SUMS[t]
        sums_wait(t)
        for q in (0, 1):
            for at_row in range(0, QUARTER, 16):
                here = pl.ds((n - 2) * HALF + q * QUARTER + at_row, 16)
                total = own_sum(t, q, at_row)
                for b in range(lo, hi):
                    at_col = nxt("z", BLOCKS[b][0]) * 512 + nxt("x", BLOCKS[b][1]) * 128
                    cols = pl.ds(pl.multiple_of(at_col, 128), 128)
                    part = total[:, (b - lo) * 128 : (b - lo + 1) * 128]
                    result[here, cols] = (middle[here, cols].astype(F32) + part).astype(BF16)

    own_copy(4).wait()
    own_copy(7).wait()
    first_norm(0)
    own_copy(5).wait()
    own_copy(6).wait()
    turn_up()
    own_copy(8).wait()
    own_copy(9).wait()
    gate_map()
    first_norm(1)
    for i in (10, 11, 12, 13):
        own_copy(i).wait()
    pl.semaphore_wait(barrier, 9)

    def sent():
        for n in range(4):
            rows_sent(n)
        for t in range(5):
            sums_sent(t)
        for i in range(4):
            weights_sent(i)

    steps = {
        "S1": first_send,
        "F1": first_forward,
        "S2": second_send,
        "F2": second_forward,
        "DA": weights_near,
        "DB": weights_far,
        "RS": rows_send,
        "R1": rows_first,
        "R2": rows_second,
        "R3": rows_third,
        "rec": recur,
        "feed": feed,
        "prod": step_product,
        "sfar": sums_far,
        "sleft": sums_left,
        "sright": sums_right,
        "near": sums_near,
        "norm2": second_norm,
        "fin": finish,
        "sent": sent,
    }
    for name, *where in ORDER:
        steps[name](*where)
    sums_sent(5)


def shards(
    resid,
    mix_gain,
    in_weight,
    conv_taps,
    recur_gate_w,
    input_gate_w,
    decay_rate,
    out_weight,
    mlp_gain,
    up_gate_w,
    up_val_w,
    ffn_taps,
    down_weight,
):
    hbm = pl.BlockSpec(memory_space=pl.ANY)
    dma = pltpu.SemaphoreType.DMA
    width = resid.shape[1]
    units = up_gate_w.shape[1]
    return pl.pallas_call(
        kernel,
        name="layer",
        out_shape=pltpu.VMEM(resid.shape, BF16),
        in_specs=[hbm] * 13,
        out_specs=pl.BlockSpec(memory_space=pltpu.VMEM),
        scratch_shapes=[
            pltpu.VMEM(resid.shape, BF16),
            pltpu.VMEM((units, 128), BF16),
            pltpu.VMEM((units, 128), BF16),
            pltpu.VMEM((1, width), F32),
            pltpu.VMEM(conv_taps.shape, F32),
            pltpu.VMEM(recur_gate_w.shape, BF16),
            pltpu.VMEM(input_gate_w.shape, BF16),
            pltpu.VMEM((1, *decay_rate.shape), F32),
            pltpu.VMEM((1, width), F32),
            pltpu.VMEM(ffn_taps.shape, F32),
            pltpu.VMEM((RING, RING, *in_weight.shape), BF16),
            pltpu.VMEM((RING, RING, *out_weight.shape), BF16),
            pltpu.VMEM((RING, RING, up_gate_w.shape[0], 2 * units), BF16),
            pltpu.VMEM((RING, RING, *down_weight.shape), BF16),
            pltpu.VMEM((4, RING, 2, 2, QUARTER, width), BF16),
            pltpu.VMEM((256, 512), BF16),
            pltpu.VMEM((4 * HALF, 256), F32),
            pltpu.VMEM((4 * HALF, 512), F32),
            pltpu.VMEM((RING, 2, 8, 256), F32),
            pltpu.VMEM((RING, 2, 8, 256), F32),
            pltpu.VMEM((2, RING, 2 * HALF, 256), BF16),
            pltpu.VMEM((4 * HALF, 2 * units), F32),
            pltpu.VMEM((RING, 2, 8, 768), F32),
            pltpu.VMEM((2, RING, 2 * HALF, units), BF16),
            pltpu.VMEM((4, RING, 2, HALF, width), BF16),
            pltpu.VMEM((4, RING, HALF, width), BF16),
            pltpu.VMEM((4, 3, 2, QUARTER, width), BF16),
            pltpu.VMEM((4, 2, QUARTER, width), BF16),
            pltpu.VMEM((4, 2, 2, QUARTER, width), BF16),
            pltpu.VMEM((SEQ, width), BF16),
            dma((4, 2)),
            dma((4, max(PIECES), 6)),
            dma((14,)),
            dma((4, 2)),
            dma((4, 14)),
            dma((6,)),
            dma((6, 4)),
            dma((6,)),
            dma((6, 6)),
        ],
        compiler_params=pltpu.CompilerParams(
            collective_id=0, has_side_effects=True, vmem_limit_bytes=56 * 1024 * 1024
        ),
    )(
        resid,
        mix_gain[None],
        in_weight,
        conv_taps,
        recur_gate_w,
        input_gate_w,
        decay_rate[None],
        out_weight,
        mlp_gain[None],
        up_gate_w.T,
        up_val_w.T,
        ffn_taps,
        down_weight,
    )


def solution(mesh):
    split = Mesh(mesh.devices.reshape(RING, RING, RING, 2), ("z", "x", "y", "c"))
    fs, tp = ("z", "x"), ("y", "c")
    rows = ("z", "x", "y", "c")
    return jax.shard_map(
        shards,
        mesh=split,
        in_specs=(
            P(rows, None),
            P(),
            P(fs, tp),
            P(None, tp),
            P(tp, None, None),
            P(tp, None, None),
            P(tp),
            P(tp, fs),
            P(),
            P(fs, tp),
            P(fs, tp),
            P(None, tp),
            P(tp, fs),
        ),
        out_specs=P(rows, None),
        check_vma=False,
    )
```

```python
import jax
import jax.numpy as jnp
from jax import lax
from jax.experimental import pallas as pl
from jax.experimental.pallas import tpu as pltpu
from jax.sharding import Mesh
from jax.sharding import PartitionSpec as P

GATE_BLOCK = 64
SEQ = 128
HALF = 64
QUARTER = 32
RING = 4
MESH = pl.DeviceIdType.MESH
BF16 = jnp.bfloat16
F32 = jnp.float32

OWN, RIGHT, LEFT, FAR, IN_RIGHT, IN_LEFT, IN_FAR = 0, 2, 4, 6, 8, 10, 12


PIECES = (4, 4, 4, 4)
X_FIRST = (2, 2, 2, 2)
DIRECT = (True, True, False, False)
SUMS = ((0, 0, 16), (1, 0, 16), (2, 0, 9), (3, 0, 9), (2, 9, 16), (3, 9, 16))
BLOCKS = tuple(
    sorted(((dz, dx) for dz in (0, 1, -1, 2) for dx in (0, 1, -1, 2)), key=lambda d: 2 in d)
)
ORDER = (
    ("S1", 3, 3),
    ("S1", 1, 2),
    ("S1", 0, 0),
    ("RS", 0),
    ("S1", 0, 2),
    ("S1", 0, 3),
    ("S1", 1, 0),
    ("S1", 0, 1),
    ("S1", 1, 1),
    ("S1", 1, 3),
    ("local",),
    ("S1", 2, 1),
    ("S1", 2, 2),
    ("F1", 0, 0),
    ("S1", 2, 0),
    ("F1", 0, 2),
    ("RS", 1),
    ("S1", 2, 3),
    ("F1", 0, 3),
    ("F1", 1, 3),
    ("F1", 0, 1),
    ("S2", 0, 0),
    ("F1", 1, 0),
    ("S2", 0, 2),
    ("S2", 0, 3),
    ("S2", 1, 3),
    ("S2", 1, 0),
    ("F1", 1, 2),
    ("S2", 1, 2),
    ("F1", 1, 1),
    ("S2", 0, 1),
    ("F1", 2, 0),
    ("F2", 0, 0),
    ("S2", 1, 1),
    ("F2", 0, 2),
    ("maps",),
    ("R1", 0),
    ("R2", 0),
    ("S1", 3, 1),
    ("F2", 0, 3),
    ("F1", 2, 3),
    ("F1", 2, 1),
    ("F1", 2, 2),
    ("F2", 0, 1),
    ("F2", 1, 1),
    ("R1", 1),
    ("F2", 1, 2),
    ("F2", 1, 0),
    ("F2", 1, 3),
    ("R2", 1),
    ("S1", 3, 0),
    ("R3", 0),
    ("S1", 3, 2),
    ("S2", 2, 0),
    ("DA", 0),
    ("DA", 1),
    ("F1", 3, 1),
    ("S2", 2, 3),
    ("DB", 0),
    ("rec", 0, 1),
    ("DB", 1),
    ("prod", 0, 1),
    ("rec", 0, 0),
    ("sfar", 0),
    ("R3", 1),
    ("F1", 3, 2),
    ("S2", 2, 1),
    ("prod", 0, 0),
    ("sleft", 0),
    ("sright", 0),
    ("S2", 2, 2),
    ("rec", 1, 1),
    ("prod", 1, 1),
    ("near", 0),
    ("rec", 1, 0),
    ("sfar", 1),
    ("prod", 1, 0),
    ("sleft", 1),
    ("F2", 2, 0),
    ("F2", 2, 3),
    ("S2", 3, 1),
    ("sright", 1),
    ("S2", 3, 2),
    ("F1", 3, 0),
    ("near", 1),
    ("F1", 3, 3),
    ("norm2", 0),
    ("RS", 2),
    ("F2", 2, 1),
    ("F2", 2, 2),
    ("R1", 2),
    ("S2", 3, 3),
    ("S2", 3, 0),
    ("norm2", 1),
    ("RS", 3),
    ("F2", 3, 2),
    ("R2", 2),
    ("R3", 2),
    ("DA", 2),
    ("DB", 2),
    ("F2", 3, 1),
    ("feed", 0, 0),
    ("F2", 3, 0),
    ("F2", 3, 3),
    ("R1", 3),
    ("DA", 3),
    ("feed", 0, 1),
    ("prod", 2, 0),
    ("prod", 2, 1),
    ("R2", 3),
    ("sfar", 2),
    ("R3", 3),
    ("DB", 3),
    ("prod", 4, 1),
    ("prod", 4, 0),
    ("sright", 2),
    ("sleft", 2),
    ("sfar", 4),
    ("feed", 1, 1),
    ("sright", 4),
    ("sleft", 4),
    ("prod", 3, 1),
    ("near", 2),
    ("prod", 5, 1),
    ("near", 4),
    ("sfar", 3),
    ("feed", 1, 0),
    ("prod", 3, 0),
    ("sfar", 5),
    ("sleft", 5),
    ("sright", 3),
    ("sleft", 3),
    ("fin", 2),
    ("prod", 5, 0),
    ("near", 3),
    ("sent",),
    ("fin", 4),
    ("sright", 5),
    ("near", 5),
    ("fin", 3),
    ("fin", 5),
)
WAITED = {0: 0, 1: 3, 3: 1}


def remote(src, dst, send_sem, recv_sem, **device):
    return pltpu.make_async_remote_copy(
        src_ref=src,
        dst_ref=dst,
        send_sem=send_sem,
        recv_sem=recv_sem,
        device_id=device,
        device_id_type=MESH,
    )


def rms_rows(wide, gain):
    scale = lax.rsqrt(jnp.mean(wide * wide, axis=-1, keepdims=True) + 1e-06)
    return (wide * scale * gain).astype(BF16)


def shifted(values, rows, by, fill):
    return jnp.where(rows >= by, pltpu.roll(values, by, axis=0), fill)


def behind(extended, by):
    return pltpu.roll(extended, by, axis=0)[8:]


def kernel(
    resid_hbm,
    mix_gain_hbm,
    in_w,
    conv_taps_hbm,
    recur_w_hbm,
    input_w_hbm,
    decay_rate_hbm,
    out_w,
    mlp_gain_hbm,
    gate_t,
    value_t,
    ffn_taps_hbm,
    down_w,
    result,
    resid,
    gate_in,
    value_in,
    mix_gain,
    conv_taps,
    recur_w,
    input_w,
    decay_rate,
    mlp_gain,
    ffn_taps,
    in_g,
    out_g,
    up_g,
    down_g,
    rows_g,
    gate_w,
    proj,
    gates,
    conv_tail,
    carry,
    recurred,
    pre,
    gate_tail,
    hidden,
    partial,
    from_core,
    to_ring,
    far_in,
    near_in,
    middle,
    w_send,
    w_recv,
    l_sem,
    g_send,
    g_recv,
    c_send,
    c_recv,
    r_send,
    r_recv,
):
    z, x, y, c = (lax.axis_index(a) for a in ("z", "x", "y", "c"))
    at = {"z": z, "x": x, "y": y}

    def nxt(axis, by):
        return lax.rem(at[axis] + (by + RING), RING)

    other = 1 - c
    y_right, y_left, y_far = nxt("y", 1), nxt("y", -1), nxt("y", 2)

    weights = ((in_w, in_g), (out_w, out_g), (None, up_g), (down_w, down_g))

    def own_copy(i):
        if i < 4:
            src, g = weights[i]
            return pltpu.make_async_copy(src, g.at[z, x], l_sem.at[i])
        src, dst = (
            (resid_hbm, resid),
            (gate_t, gate_in),
            (value_t, value_in),
            (mix_gain_hbm, mix_gain),
            (recur_w_hbm, recur_w),
            (input_w_hbm, input_w),
            (conv_taps_hbm, conv_taps),
            (decay_rate_hbm, decay_rate),
            (mlp_gain_hbm, mlp_gain),
            (ffn_taps_hbm, ffn_taps),
        )[i - 4]
        return pltpu.make_async_copy(src, dst, l_sem.at[i])

    for i in (4, 7, 5, 6, 8, 9, 10, 11, 12, 13, 0, 1, 3):
        own_copy(i).start()

    barrier = pltpu.get_barrier_semaphore()
    for axis in ("z", "x", "y"):
        for by in (1, -1) if axis == "y" else (1, -1, 2):
            pl.semaphore_signal(
                barrier, inc=1, device_id={axis: nxt(axis, by)}, device_id_type=MESH
            )
    pl.semaphore_signal(barrier, inc=1, device_id={"c": other}, device_id_type=MESH)

    def piece(i, p):
        rows = weights[i][1].shape[2] // PIECES[i]
        return pl.ds(p * rows, rows)

    def axes_of(i, p):
        return ("x", "z") if p < X_FIRST[i] else ("z", "x")

    def slot(i, p, axis, by):
        g = weights[i][1]
        if axis == "x":
            return g.at[z, nxt("x", by), piece(i, p)]
        return g.at[nxt("z", by), x, piece(i, p)]

    def line(i, p, axis, by):
        g = weights[i][1]
        if axis == "z":
            return g.at[nxt("z", by), :, piece(i, p)]
        return g.at[:, nxt("x", by), piece(i, p)]

    def w_copy(i, p, src, dst, k, axis, by):
        return remote(
            src, dst, w_send.at[i, k // 3], w_recv.at[i, p, k], **{axis: nxt(axis, by)}
        )

    def first_send(i, p):
        src = weights[i][0]
        axis = axes_of(i, p)[0]
        here = slot(i, p, axis, 0)
        for k, by in ((0, 1), (1, -1), (2, 2))[: 3 if DIRECT[i] else 2]:
            w_copy(i, p, here if src is None else src.at[piece(i, p)], here, k, axis, by).start()

    def first_wait(i, p, k):
        axis = axes_of(i, p)[0]
        there = slot(i, p, axis, (-1, 1, 2)[k])
        w_copy(i, p, there, there, k, axis, 1).wait_recv()

    def first_forward(i, p):
        axis = axes_of(i, p)[0]
        k = p % 2
        first_wait(i, p, k)
        by = 1 if k == 0 else -1
        there = slot(i, p, axis, -by)
        if not DIRECT[i]:
            w_copy(i, p, there, there, 2, axis, by).start()

    def second_send(i, p):
        if p == WAITED.get(i):
            own_copy(i).wait()
        axis = axes_of(i, p)[1]
        first_wait(i, p, 1 - p % 2)
        first_wait(i, p, 2)
        here = line(i, p, axis, 0)
        for k, by in ((3, 1), (4, -1)):
            w_copy(i, p, here, here, k, axis, by).start()

    def second_wait(i, p, k):
        axis = axes_of(i, p)[1]
        there = line(i, p, axis, (-1, 1, 2)[k - 3])
        w_copy(i, p, there, there, k, axis, 1).wait_recv()

    def second_forward(i, p):
        axis = axes_of(i, p)[1]
        k = 3 + p % 2
        second_wait(i, p, k)
        by = 1 if k == 3 else -1
        there = line(i, p, axis, -by)
        w_copy(i, p, there, there, 5, axis, by).start()

    def weights_near(i):
        for p in range(PIECES[i]):
            second_wait(i, p, 4 - p % 2)

    def weights_far(i):
        for p in range(PIECES[i]):
            second_wait(i, p, 5)

    def all_sent(ref, sem):
        pltpu.make_async_copy(ref, ref, sem).wait()

    def weights_sent(i):
        g = weights[i][1]
        all_sent(g.at[0, pl.ds(0, 3)], w_send.at[i, 0])
        all_sent(g.at[pl.ds(0, 3)], w_send.at[i, 1])

    def g_copy(n, yq, cq, q, s, r, **device):
        ref = rows_g.at[n, yq, cq, q]
        return remote(ref, ref, g_send.at[n, s // 12], g_recv.at[n, r], **device)

    def rows_wait(n, yq, cq, q, r):
        g_copy(n, yq, cq, q, 0, r, c=other).wait_recv()

    def rows_send(n):
        for q in (0, 1):
            g_copy(n, y, c, q, q, IN_LEFT + q, y=y_right).start()
            g_copy(n, y, c, 1 - q, 2 + 1 - q, IN_RIGHT + 1 - q, y=y_left).start()
            g_copy(n, y, c, q, 4 + q, OWN + q, c=other).start()

    def rows_first(n):
        rows_wait(n, y_left, c, 0, IN_LEFT)
        g_copy(n, y_left, c, 0, 6, IN_FAR, y=y_right).start()
        g_copy(n, y_left, c, 0, 8, LEFT, c=other).start()
        rows_wait(n, y_right, c, 1, IN_RIGHT + 1)
        g_copy(n, y_right, c, 1, 7, IN_FAR + 1, y=y_left).start()
        g_copy(n, y_right, c, 1, 11, RIGHT + 1, c=other).start()

    def rows_second(n):
        rows_wait(n, y_left, c, 1, IN_LEFT + 1)
        g_copy(n, y_left, c, 1, 9, LEFT + 1, c=other).start()
        rows_wait(n, y_right, c, 0, IN_RIGHT)
        g_copy(n, y_right, c, 0, 10, RIGHT, c=other).start()

    def rows_third(n):
        for q in (0, 1):
            rows_wait(n, y_far, c, q, IN_FAR + q)
            g_copy(n, y_far, c, q, 12 + q, FAR + q, c=other).start()

    def rows_sent(n):
        all_sent(rows_g.at[n, pl.ds(0, 3)], g_send.at[n, 0])
        all_sent(rows_g.at[n, 3, 0], g_send.at[n, 1])

    def group(g):
        return (y, y_right) if g == 0 else (y_left, y_far)

    def group_rows(n, g):
        for j, yq in enumerate(group(g)):
            for q in (0, 1):
                rows_wait(n, yq, other, q, 4 * g + 2 * j + q)
        return jnp.concatenate([rows_g[n, yq].reshape(2 * HALF, -1) for yq in group(g)], axis=0)

    def place(t):
        n, lo, hi = SUMS[t]
        return n, pl.ds(lo * 128, (hi - lo) * 128)

    def core_copy(t, yq, k):
        n, cols = place(t)
        return remote(
            partial.at[n, yq, other, :, cols],
            from_core.at[n, yq, :, cols],
            c_send.at[t],
            c_recv.at[t, k],
            c=other,
        )

    def ring_copy(t, j, q, k, side, **device):
        n, cols = place(t)
        there = far_in.at[n, q, :, cols] if side is None else near_in.at[n, side, q, :, cols]
        return remote(to_ring.at[n, j, q, :, cols], there, r_send.at[t], r_recv.at[t, k], **device)

    def chip_sum(t, yq, at_row):
        n, cols = place(t)
        rows = pl.ds(at_row, 16)
        return partial[n, yq, c, rows, cols].astype(F32) + from_core[n, yq, rows, cols].astype(F32)

    def fill_ring(t, j, q, yq, far=False):
        n, cols = place(t)
        for at_row in range(0, QUARTER, 16):
            total = chip_sum(t, yq, q * QUARTER + at_row)
            if far:
                total = total + far_in[n, q, at_row : at_row + 16, cols].astype(F32)
            to_ring[n, j, q, at_row : at_row + 16, cols] = total.astype(BF16)

    def sums_far(t):
        core_copy(t, y_far, 0).wait_recv()
        fill_ring(t, 0, 0, y_far)
        ring_copy(t, 0, 0, 0, None, y=y_right).start()
        fill_ring(t, 0, 1, y_far)
        ring_copy(t, 0, 1, 1, None, y=y_left).start()

    def sums_left(t):
        core_copy(t, y_left, 1).wait_recv()
        fill_ring(t, 1, 0, y_left)
        ring_copy(t, 1, 0, 2, 1, y=y_left).start()

    def sums_right(t):
        core_copy(t, y_right, 2).wait_recv()
        fill_ring(t, 2, 1, y_right)
        ring_copy(t, 2, 1, 3, 0, y=y_right).start()

    def sums_near(t):
        ring_copy(t, 0, 0, 0, None, y=y_right).wait_recv()
        fill_ring(t, 2, 0, y_right, True)
        ring_copy(t, 2, 0, 4, 0, y=y_right).start()
        ring_copy(t, 0, 1, 1, None, y=y_left).wait_recv()
        fill_ring(t, 1, 1, y_left, True)
        ring_copy(t, 1, 1, 5, 1, y=y_left).start()

    def sums_sent(t):
        n, cols = place(t)
        all_sent(from_core.at[n, :, :, cols], c_send.at[t])
        all_sent(to_ring.at[n, :, :, :, cols], r_send.at[t])

    def sums_wait(t):
        core_copy(t, y, 3).wait_recv()
        for side in (0, 1):
            for q in (0, 1):
                k = ((4, 3), (2, 5))[side][q]
                ring_copy(t, 0, q, k, side, y=y_right).wait_recv()

    def own_sum(t, q, at_row):
        n, cols = place(t)
        total = chip_sum(t, y, q * QUARTER + at_row)
        for side in (0, 1):
            total = total + near_in[n, side, q, at_row : at_row + 16, cols].astype(F32)
        return total

    def first_norm(h):
        for q in (0, 1):
            for at_row in range(0, QUARTER, 16):
                here = h * HALF + q * QUARTER + at_row
                wide = resid[here : here + 16, :].astype(F32)
                rows_g[h, y, c, q, at_row : at_row + 16, :] = rms_rows(wide, mix_gain[...])

    def gate_map():
        gate_w[...] = jnp.zeros_like(gate_w)
        for n in range(recur_w.shape[0]):
            block = slice(n * GATE_BLOCK, (n + 1) * GATE_BLOCK)
            gate_w[block, block] = recur_w[n]
            block_two = slice(256 + n * GATE_BLOCK, 256 + (n + 1) * GATE_BLOCK)
            gate_w[block, block_two] = input_w[n]

    def turn_up():
        for b in range(11):
            if b < 5:
                tile = gate_in[b * 128 : (b + 1) * 128, :]
            elif b < 10:
                tile = value_in[(b - 5) * 128 : (b - 4) * 128, :]
            else:
                tile = jnp.concatenate([gate_in[640:704, :], value_in[640:704, :]], axis=0)
            up_g[z, x, :, b * 128 : (b + 1) * 128] = tile.astype(F32).T.astype(BF16)

    def recur(h, g):
        w = in_g[...].reshape(-1, 256)
        proj[...] = jnp.dot(group_rows(h, g), w, preferred_element_type=F32)
        taps = conv_taps[...]
        blocks = [(j, s) for j in range(2) for s in range(2)]
        for j, s in blocks:
            yq = group(g)[j]
            rows = slice((2 * j + s) * HALF, (2 * j + s + 1) * HALF)
            wide = proj[rows, :].astype(BF16).astype(F32)
            before = jnp.zeros((8, 256), F32) if h == 0 else conv_tail[yq, s]
            if h == 0:
                conv_tail[yq, s] = wide[HALF - 8 :]
            extended = jnp.concatenate([before, wide], axis=0)
            conv = behind(extended, 3) * taps[0:1]
            conv = conv + behind(extended, 2) * taps[1:2]
            conv = conv + behind(extended, 1) * taps[2:3]
            proj[rows, :] = conv + wide * taps[3:4]
        gates[...] = jnp.dot(proj[...].astype(BF16), gate_w[...], preferred_element_type=F32)
        for j, s in blocks:
            yq = group(g)[j]
            rows = slice((2 * j + s) * HALF, (2 * j + s + 1) * HALF)
            for b in range(2):
                lanes = slice(b * 128, (b + 1) * 128)
                lanes2 = slice(256 + b * 128, 256 + (b + 1) * 128)
                rgate = jax.nn.sigmoid(gates[rows, lanes])
                igate = jax.nn.sigmoid(gates[rows, lanes2])
                a = 8.0 * rgate * decay_rate[:, lanes]
                decay = jnp.exp(-a)
                a2 = a * a
                series = 1.0 + a2 * (1.0 / 6) * (1.0 + a2 * (1.0 / 20) * (1.0 + a2 * (1.0 / 42)))
                left_over = jnp.where(a < 0.3, 2.0 * decay * (a * series), 1.0 - decay * decay)
                state = jnp.sqrt(left_over) * (igate * proj[rows, lanes])
                pos = lax.broadcasted_iota(jnp.int32, state.shape, 0)
                if h == 1:
                    state = state + jnp.where(pos == 0, decay * carry[yq, s, 0:1, lanes], 0.0)
                by = 1
                while by < HALF:
                    state = decay * shifted(state, pos, by, 0.0) + state
                    if 2 * by < HALF:
                        decay = decay * shifted(decay, pos, by, 1.0)
                    by *= 2
                if h == 0:
                    carry[yq, s, 0:1, lanes] = state[HALF - 1 :]
                recurred[h, yq, s * HALF : (s + 1) * HALF, lanes] = state.astype(BF16)

    def step_product(t, g):
        n, lo, hi = SUMS[t]
        left, table = (recurred, out_g) if n < 2 else (hidden, down_g)
        rows = jnp.concatenate([left[n % 2, yq] for yq in group(g)], axis=0)
        for b in range(lo, hi, 4):
            end = min(b + 4, hi)
            w = []
            for d in range(b, end):
                if n < 2:
                    w.append(table[d // RING, d % RING])
                else:
                    w.append(table[nxt("z", BLOCKS[d][0]), nxt("x", BLOCKS[d][1])])
            term = jnp.dot(rows, jnp.concatenate(w, axis=1), preferred_element_type=F32)
            term = term.astype(BF16)
            for j, yq in enumerate(group(g)):
                for s in range(2):
                    at_row = (2 * j + s) * HALF
                    partial[n, yq, s, :, b * 128 : end * 128] = term[at_row : at_row + HALF]
        for j, k in ((1, 2), (0, 3)) if g == 0 else ((1, 0), (0, 1)):
            core_copy(t, group(g)[j], k).start()

    def second_norm(h):
        sums_wait(h)
        for q in (0, 1):
            for at_row in range(0, QUARTER, 16):
                lo = h * HALF + q * QUARTER + at_row
                here = slice(lo, lo + 16)
                mid = (resid[here, :].astype(F32) + own_sum(h, q, at_row)).astype(BF16)
                middle[here, :] = mid
                out = rms_rows(mid.astype(F32), mlp_gain[...])
                rows_g[2 + h, y, c, q, at_row : at_row + 16, :] = out

    def gated(extended, value, taps):
        conv = behind(extended, 2) * taps[0:1]
        conv = conv + behind(extended, 1) * taps[1:2]
        conv = conv + extended[8:] * taps[2:3]
        return (conv / (1.0 + jnp.exp(-conv)) * value).astype(BF16)

    def feed(h, g):
        w = up_g[...].reshape(-1, 1408)
        pre[...] = jnp.dot(group_rows(2 + h, g), w, preferred_element_type=F32)
        for j in range(2):
            yq = group(g)[j]
            for s in range(2):
                rows = slice((2 * j + s) * HALF, (2 * j + s + 1) * HALF)
                out = slice(s * HALF, (s + 1) * HALF)
                for b in range(6):
                    lanes = slice(b * 128, (b + 1) * 128)
                    if b < 5:
                        gate = pre[rows, lanes].astype(BF16).astype(F32)
                        value = pre[rows, 640 + b * 128 : 640 + (b + 1) * 128]
                        value = value.astype(BF16).astype(F32)
                        taps = ffn_taps[:, lanes]
                    else:
                        gate = pre[rows, 1280:1408].astype(BF16).astype(F32)
                        value = pltpu.roll(gate, 64, axis=1)
                        taps = jnp.concatenate([ffn_taps[:, 640:704], jnp.zeros((3, 64), F32)], axis=1)
                    before = jnp.zeros((8, 128), F32) if h == 0 else gate_tail[yq, s, :, lanes]
                    if h == 0:
                        gate_tail[yq, s, :, lanes] = gate[HALF - 8 :]
                    unit = gated(jnp.concatenate([before, gate], axis=0), value, taps)
                    if b < 5:
                        hidden[h, yq, out, lanes] = unit
                    else:
                        hidden[h, yq, out, 640:704] = unit[:, :64]

    def finish(t):
        n, lo, hi = SUMS[t]
        sums_wait(t)
        for q in (0, 1):
            for at_row in range(0, QUARTER, 16):
                here = pl.ds((n - 2) * HALF + q * QUARTER + at_row, 16)
                total = own_sum(t, q, at_row)
                for b in range(lo, hi):
                    at_col = nxt("z", BLOCKS[b][0]) * 512 + nxt("x", BLOCKS[b][1]) * 128
                    cols = pl.ds(pl.multiple_of(at_col, 128), 128)
                    part = total[:, (b - lo) * 128 : (b - lo + 1) * 128]
                    result[here, cols] = (middle[here, cols].astype(F32) + part).astype(BF16)

    own_copy(4).wait()
    own_copy(7).wait()
    first_norm(0)
    pl.semaphore_wait(barrier, 9)

    def local():
        own_copy(5).wait()
        own_copy(6).wait()
        turn_up()
        first_norm(1)

    def maps():
        for i in (8, 9, 10, 11, 12, 13):
            own_copy(i).wait()
        gate_map()

    def sent():
        for n in range(4):
            rows_sent(n)
        for t in range(5):
            sums_sent(t)
        for i in range(4):
            weights_sent(i)

    steps = {
        "local": local,
        "maps": maps,
        "S1": first_send,
        "F1": first_forward,
        "S2": second_send,
        "F2": second_forward,
        "DA": weights_near,
        "DB": weights_far,
        "RS": rows_send,
        "R1": rows_first,
        "R2": rows_second,
        "R3": rows_third,
        "rec": recur,
        "feed": feed,
        "prod": step_product,
        "sfar": sums_far,
        "sleft": sums_left,
        "sright": sums_right,
        "near": sums_near,
        "norm2": second_norm,
        "fin": finish,
        "sent": sent,
    }
    for name, *where in ORDER:
        steps[name](*where)
    sums_sent(5)


def shards(
    resid,
    mix_gain,
    in_weight,
    conv_taps,
    recur_gate_w,
    input_gate_w,
    decay_rate,
    out_weight,
    mlp_gain,
    up_gate_w,
    up_val_w,
    ffn_taps,
    down_weight,
):
    hbm = pl.BlockSpec(memory_space=pl.ANY)
    dma = pltpu.SemaphoreType.DMA
    width = resid.shape[1]
    units = up_gate_w.shape[1]
    return pl.pallas_call(
        kernel,
        name="layer",
        out_shape=pltpu.VMEM(resid.shape, BF16),
        in_specs=[hbm] * 13,
        out_specs=pl.BlockSpec(memory_space=pltpu.VMEM),
        scratch_shapes=[
            pltpu.VMEM(resid.shape, BF16),
            pltpu.VMEM((units, 128), BF16),
            pltpu.VMEM((units, 128), BF16),
            pltpu.VMEM((1, width), F32),
            pltpu.VMEM(conv_taps.shape, F32),
            pltpu.VMEM(recur_gate_w.shape, BF16),
            pltpu.VMEM(input_gate_w.shape, BF16),
            pltpu.VMEM((1, *decay_rate.shape), F32),
            pltpu.VMEM((1, width), F32),
            pltpu.VMEM(ffn_taps.shape, F32),
            pltpu.VMEM((RING, RING, *in_weight.shape), BF16),
            pltpu.VMEM((RING, RING, *out_weight.shape), BF16),
            pltpu.VMEM((RING, RING, up_gate_w.shape[0], 2 * units), BF16),
            pltpu.VMEM((RING, RING, *down_weight.shape), BF16),
            pltpu.VMEM((4, RING, 2, 2, QUARTER, width), BF16),
            pltpu.VMEM((256, 512), BF16),
            pltpu.VMEM((4 * HALF, 256), F32),
            pltpu.VMEM((4 * HALF, 512), F32),
            pltpu.VMEM((RING, 2, 8, 256), F32),
            pltpu.VMEM((RING, 2, 8, 256), F32),
            pltpu.VMEM((2, RING, 2 * HALF, 256), BF16),
            pltpu.VMEM((4 * HALF, 2 * units), F32),
            pltpu.VMEM((RING, 2, 8, 768), F32),
            pltpu.VMEM((2, RING, 2 * HALF, units), BF16),
            pltpu.VMEM((4, RING, 2, HALF, width), BF16),
            pltpu.VMEM((4, RING, HALF, width), BF16),
            pltpu.VMEM((4, 3, 2, QUARTER, width), BF16),
            pltpu.VMEM((4, 2, QUARTER, width), BF16),
            pltpu.VMEM((4, 2, 2, QUARTER, width), BF16),
            pltpu.VMEM((SEQ, width), BF16),
            dma((4, 2)),
            dma((4, max(PIECES), 6)),
            dma((14,)),
            dma((4, 2)),
            dma((4, 14)),
            dma((6,)),
            dma((6, 4)),
            dma((6,)),
            dma((6, 6)),
        ],
        compiler_params=pltpu.CompilerParams(
            collective_id=0, has_side_effects=True, vmem_limit_bytes=56 * 1024 * 1024
        ),
    )(
        resid,
        mix_gain[None],
        in_weight,
        conv_taps,
        recur_gate_w,
        input_gate_w,
        decay_rate[None],
        out_weight,
        mlp_gain[None],
        up_gate_w.T,
        up_val_w.T,
        ffn_taps,
        down_weight,
    )


def solution(mesh):
    split = Mesh(mesh.devices.reshape(RING, RING, RING, 2), ("z", "x", "y", "c"))
    fs, tp = ("z", "x"), ("y", "c")
    rows = ("z", "x", "y", "c")
    return jax.shard_map(
        shards,
        mesh=split,
        in_specs=(
            P(rows, None),
            P(),
            P(fs, tp),
            P(None, tp),
            P(tp, None, None),
            P(tp, None, None),
            P(tp),
            P(tp, fs),
            P(),
            P(fs, tp),
            P(fs, tp),
            P(None, tp),
            P(tp, fs),
        ),
        out_specs=P(rows, None),
        check_vma=False,
    )
```
